256 devices in a mesh: ep: 32 (over z, x), tp: 8 (over y, core).
Axes of the slice: x: 4, y: 4, z: 8, core: 2. Of those that a mesh axis runs over, the one named last changes fastest.
Arguments:
- hidden: bfloat16 [1024, 4096], P('ep', 'tp'), may hold values from -6 to 6
- norm_gain: float32 [4096], P('tp'), may hold values from 0.1 to 1.9
- expert_ids: int32 [1024, 8], P('ep'), may hold values from 0 to 63, as said below
- route_weights: float32 [1024, 8], P('ep'), may hold values from 0.1 to 1
- lengths: int32 [128], P('ep'), may hold values from 1 to 8, as said below
- gate_proj: bfloat16 [64, 4096, 1024], P('ep', None, 'tp'), may hold values from -0.09375 to 0.09375
- up_proj: bfloat16 [64, 4096, 1024], P('ep', None, 'tp'), may hold values from -0.09375 to 0.09375
- down_proj: bfloat16 [64, 1024, 4096], P('ep', 'tp'), may hold values from -0.1875 to 0.1875
- shared_gate: bfloat16 [4096, 1024], P(None, 'tp'), may hold values from -0.09375 to 0.09375
- shared_up: bfloat16 [4096, 1024], P(None, 'tp'), may hold values from -0.09375 to 0.09375
- shared_down: bfloat16 [1024, 4096], P('tp'), may hold values from -0.1875 to 0.1875
Outputs:
- mixed: bfloat16 [1024, 4096], P('ep', 'tp')
The draws below stay inside these ranges and needn't reach their ends.
Inputs may be any that keep to these rules, and one draw needn't show every extreme that they name: `expert_ids`: among the 32 rows of one index of ep (an aligned block), no expert is named more than 12 times, and in every block one expert is named exactly 12 times; each row names 8 different experts. `lengths`: each sequence has 1 to 8 live slots; on some index of ep all 4 sequences have 8 live slots.
All inputs are finite; a program needn't handle non-finite values.
Results may differ from the reference program's by a relative error of at most 0.015.
Values may be sent and summed in bfloat16 or wider, within the bound.
A program may use at most 128 MiB of HBM per device.

```python
import jax
import jax.numpy as jnp
import numpy as np
from jax import lax

D = 4096
FF = 1024
SFF = 1024
TOP = 8
SPAN = 8
SEQ_DEV = 4
EXPERTS = 64
SEQS = 128
SLOTS_DEV = 32
ROWS = 1024
CAP = 12
N_EP = 32


def rank_counts():
    others = EXPERTS - 1
    tier_weights = []
    for rank in range(others):
        if rank < others // 8:
            tier_weights.append(3)
        elif rank < others // 2:
            tier_weights.append(2)
        else:
            tier_weights.append(1)
    leftover = SLOTS_DEV * TOP - CAP
    counts = [0] * others
    height = 0
    while leftover > 0:
        height = height + 1
        for rank in range(others):
            if leftover > 0:
                target = min(CAP, tier_weights[rank] * height)
                added = min(max(target - counts[rank], 0), leftover)
                counts[rank] = counts[rank] + added
                leftover = leftover - added
    return [CAP] + counts


def one_block(block_key, rank_table):
    order_key, row_key, column_key = jax.random.split(block_key, 3)
    label_order = jax.random.permutation(order_key, EXPERTS).astype(jnp.int32)
    labels = label_order[rank_table]
    chosen = labels.reshape(TOP, SLOTS_DEV).T
    row_order = jax.random.permutation(row_key, SLOTS_DEV)
    chosen = chosen[row_order]
    scores = jax.random.randint(column_key, (SLOTS_DEV, TOP), 0, 1 << 20) * TOP + jnp.arange(TOP, dtype=jnp.int32)[None, :]
    column_order = jnp.argsort(scores, axis=1, stable=True)
    return jnp.take_along_axis(chosen, column_order, axis=1).astype(jnp.int32)


def draw_expert_ids(key, part):
    block_count = SEQS // SEQ_DEV
    rank_table = jnp.asarray(np.repeat(np.arange(EXPERTS), np.array(rank_counts())), dtype=jnp.int32)
    block_keys = jax.random.split(jax.random.fold_in(key, 11), block_count)
    blocks = jax.vmap(lambda single_key: one_block(single_key, rank_table))(block_keys)
    return blocks.reshape(block_count * SLOTS_DEV, TOP).astype(jnp.int32)


def draw_lengths(key, part):
    short_key, long_key, pick_key, block_key = jax.random.split(jax.random.fold_in(key, 23), 4)
    short_len = jax.random.randint(short_key, (SEQS,), 1, 3)
    long_len = jax.random.randint(long_key, (SEQS,), SPAN // 2 + 1, SPAN + 1)
    picked = jax.random.randint(pick_key, (SEQS,), 0, 4) == 0
    drawn = jnp.where(picked, long_len, short_len)
    full_block = jax.random.randint(block_key, (), 0, SEQS // SEQ_DEV)
    owner = jnp.arange(SEQS, dtype=jnp.int32) // SEQ_DEV
    return jnp.where(owner == full_block, SPAN, drawn).astype(jnp.int32)


def level_of(own_key, extent, shards, low, top_value):
    def one(dim, blocks):
        heights = jax.random.uniform(jax.random.fold_in(jax.random.fold_in(own_key, 6), dim), (blocks,), jnp.float32, low / len(shards), top_value / len(shards))
        return jnp.repeat(jnp.exp(heights), extent[dim] // blocks).reshape((-1,) + (1,) * (len(extent) - dim - 1))

    gain = one(*shards[0])
    for cut in shards[1:]:
        gain = gain * one(*cut)
    return gain


def noise(key, shape, spread, bound, cuts=(), held_as=jnp.bfloat16):
    gain = level_of(key, shape, cuts, -0.22, 0.18) if cuts else 1.0
    entries = jax.random.normal(key, shape, jnp.float32) * spread * gain
    return jnp.minimum(jnp.maximum(entries, -bound), bound).astype(held_as)


def setup_inputs(seed: int = 0) -> dict:
    splits = jax.random.split(jax.random.key(seed), 12)
    return {
        "hidden": noise(splits[0], (ROWS, D), 1.0, 6.0, ((0, 32), (1, 8))),
        "norm_gain": jnp.clip(1.0 + 0.18 * jax.random.normal(splits[1], (D,), jnp.float32), 0.1, 1.9),
        "expert_ids": draw_expert_ids(jax.random.fold_in(splits[11], 71), 0),
        "route_weights": jnp.clip(0.1 + 0.9 * jax.random.uniform(splits[3], (ROWS, TOP), jnp.float32) ** level_of(splits[3], (ROWS, TOP), ((0, 32),), -0.2, 0.2), 0.1, 1.0),
        "lengths": draw_lengths(jax.random.fold_in(splits[11], 71), 0),
        "gate_proj": noise(splits[5], (EXPERTS, D, FF), D ** -0.5, 0.09375, ((0, 32), (2, 8))),
        "up_proj": noise(splits[6], (EXPERTS, D, FF), D ** -0.5, 0.09375, ((0, 32), (2, 8))),
        "down_proj": noise(splits[7], (EXPERTS, FF, D), FF ** -0.5, 0.1875, ((0, 32), (1, 8))),
        "shared_gate": noise(splits[8], (D, SFF), D ** -0.5, 0.09375, ((1, 8),)),
        "shared_up": noise(splits[9], (D, SFF), D ** -0.5, 0.09375, ((1, 8),)),
        "shared_down": noise(splits[10], (SFF, D), SFF ** -0.5, 0.1875, ((0, 8),)),
    }


epsilon = 1e-06

def reference(hidden, norm_gain, expert_ids, route_weights, lengths, gate_proj, up_proj, down_proj, shared_gate, shared_up, shared_down):
    row_count = hidden.shape[0]
    values = hidden.astype(jnp.float32)
    normed = (values * lax.rsqrt(lax.optimization_barrier(jnp.mean(values * values, axis=1, keepdims=True)) + epsilon) * norm_gain[None, :]).astype(jnp.bfloat16)
    offsets = jnp.arange(row_count, dtype=jnp.int32) % SPAN
    is_live = offsets < jnp.repeat(lengths, SPAN)
    mixing = jnp.where(is_live[:, None], route_weights, 0.0)
    expert_range = jnp.arange(EXPERTS, dtype=jnp.int32)
    is_named = (expert_ids[:, :, None] == expert_range[None, None, :]) & is_live[:, None, None]
    by_expert = lax.optimization_barrier(jnp.sum(jnp.where(is_named, mixing[:, :, None], 0.0), axis=1))
    hit_any = jnp.any(is_named, axis=1)
    row_order = (row_count - jnp.arange(row_count, dtype=jnp.int32)).astype(jnp.int32)
    pick_count = min(row_count, N_EP * CAP)

    def one_expert(accumulated, per_expert):
        hit_column, mix_column, w_gate, w_up, w_down = per_expert
        score = jnp.where(hit_column, row_order, 0).astype(jnp.int32)
        _, chosen = lax.top_k(score, pick_count)
        row_inputs = normed[chosen]
        gate_value = jnp.dot(row_inputs, w_gate, preferred_element_type=jnp.float32)
        up_value = jnp.dot(row_inputs, w_up, preferred_element_type=jnp.float32)
        inner_value = (jax.nn.silu(gate_value) * up_value).astype(jnp.bfloat16)
        result = jnp.dot(inner_value, w_down, preferred_element_type=jnp.float32)
        return (accumulated.at[chosen].add(mix_column[chosen][:, None] * result), None)
    start_value = jnp.zeros((row_count, hidden.shape[1]), jnp.float32)
    routed, _ = lax.scan(one_expert, start_value, (hit_any.T, by_expert.T, gate_proj, up_proj, down_proj))
    shared_inner = (jax.nn.silu(jnp.dot(normed, shared_gate, preferred_element_type=jnp.float32)) * jnp.dot(normed, shared_up, preferred_element_type=jnp.float32)).astype(jnp.bfloat16)
    shared = jnp.dot(shared_inner, shared_down, preferred_element_type=jnp.float32)
    return jnp.where(is_live[:, None], routed + shared, 0.0).astype(jnp.bfloat16)
```

```python
import functools

import jax
import jax.numpy as jnp
from jax import lax
from jax.experimental import pallas as pl
from jax.experimental.pallas import tpu as pltpu
from jax.sharding import PartitionSpec as P

MESH = pl.DeviceIdType.MESH
EPS = 1e-06
NZ, NX, NY = 8, 4, 4
BLK = 16
HALF = 512
F32, BF16 = jnp.float32, jnp.bfloat16
SEQ = (0, 1, 7, 2, 6, 3, 5, 4)
POS = {dz: i for i, dz in enumerate(SEQ)}


class Ids:
    def __init__(self):
        self.table, self.count = {}, 0

    def at(self, *key):
        if key not in self.table:
            self.table[key] = self.count
            self.count += 1
        return self.table[key]


def build_ids():
    ids = Ids()
    for p in range(NZ):
        for h in range(2):
            ids.at("z", p, h)
    for p in range(NZ):
        ids.at("zr", p)
        for r in (1, 2, 3):
            ids.at("br", p, r)
            for h in range(2):
                for stage in ("ab", "ac", "rc", "rb"):
                    ids.at(stage, p, h, r)
        for c in range(2):
            ids.at("rz", p, c)
    for k in range(8):
        ids.at("gain", k)
    for k in range(9):
        ids.at("w", k)
    return ids


IDS = build_ids()


def kernel(
    hidden_ref, gain_ref, eid_ref, rw_ref, len_ref, gate_ref, up_ref, down_ref, sgate_ref, sup_ref, sdown_ref,
    out_ref,
    hbuf, pbuf, rbuf, rown, gbuf, hn, inner, wgu, wd, wsgu, wsd, fc0, fc1, fb, zb, lsem, ssem, rsem,
):
    ep, tp = lax.axis_index("ep"), lax.axis_index("tp")
    z, x = ep // NX, ep % NX
    y, core = tp // 2, tp % 2
    other = 1 - core

    def dev(dz=0, dx=0, dy=0, c=None):
        c = core if c is None else c
        return (((z + dz) % NZ) * NX + (x + dx) % NX, ((y + dy) % NY) * 2 + c)

    started = []

    def push(src, dst, key, to, add=0):
        i = IDS.at(*key) + add
        cp = pltpu.make_async_remote_copy(
            src_ref=src, dst_ref=dst, send_sem=ssem.at[i], recv_sem=rsem.at[i], device_id=to, device_id_type=MESH
        )
        cp.start()
        started.append(cp)

    def arrive(dst, key, add=0):
        i = IDS.at(*key) + add
        pltpu.make_async_remote_copy(
            src_ref=dst, dst_ref=dst, send_sem=ssem.at[i], recv_sem=rsem.at[i], device_id=dev(c=other), device_id_type=MESH
        ).wait_recv()

    def lanes(first):
        return pl.ds(pl.multiple_of(first + core * 128, 128), 128)

    weights = []
    for e in range(2):
        weights.append((gate_ref.at[e], wgu.at[:, lanes(e * 256)]))
        weights.append((up_ref.at[e], wgu.at[:, lanes(512 + e * 256)]))
    weights.append((sgate_ref, wsgu.at[:, lanes(0)]))
    weights.append((sup_ref, wsgu.at[:, lanes(256)]))
    for e in range(2):
        weights.append((down_ref.at[e], wd.at[lanes(e * 256), :]))
    weights.append((sdown_ref, wsd.at[lanes(0), :]))
    local = [pltpu.make_async_copy(s, d, lsem.at[k]) for k, (s, d) in enumerate(weights)]
    for cp in local:
        cp.start()

    barrier = pltpu.get_barrier_semaphore()
    peers = [dev(dz=o, c=c) for o in range(1, NZ) for c in range(2)] + [dev(c=other)]
    peers += [dev(dy=o, c=c) for o in range(1, NY) for c in range(2)]
    peers += [dev(dx=1), dev(dx=-1 + NX)]
    for peer in peers:
        pl.semaphore_signal(barrier, inc=1, device_id=peer, device_id_type=MESH)

    lane = lax.broadcasted_iota(jnp.int32, (32, 128), 1)
    row = lax.broadcasted_iota(jnp.int32, (32, 128), 0)
    seq_len = jnp.zeros((32, 128), jnp.int32)
    for q in range(4):
        seq_len = jnp.where(row // 8 == q, len_ref[q], seq_len)
    live = row % 8 < seq_len
    mix = jnp.zeros((32, 128), F32)
    for k in range(8):
        mix = mix + jnp.where(eid_ref[:, k : k + 1] == lane % 64, rw_ref[:, k : k + 1], 0.0)
    mix = jnp.where(live, mix, 0.0)
    high = mix.astype(BF16).astype(F32)
    terms = jnp.where(lane < 64, high, mix - high).astype(BF16)
    rown[...] = terms.reshape(2, BLK, 128)
    rbuf[0, 0:BLK, :] = rown[core]
    gbuf[tp] = gain_ref[...]
    hbuf[core, 0, 0:BLK, 0:HALF] = hidden_ref[core]

    pl.semaphore_wait(barrier, len(peers))

    for o in (1, 7, 2, 6, 3, 5, 4):
        p = POS[(-o) % NZ]
        if o == 1:
            push(hidden_ref.at[other], hbuf.at[core, 0, 0:BLK, 0:HALF], ("z", 0, 0), dev(c=other), core)
        for c in range(2):
            push(hidden_ref.at[c], hbuf.at[core, p, 0:BLK, 0:HALF], ("z", p, 0), dev(dz=o, c=c), core)
        push(rown.at[core], rbuf.at[p, 0:BLK, :], ("zr", p), dev(dz=o))
    for k, (s, d) in enumerate(weights):
        if k < 4:
            push(s, d, ("w", k), dev(c=other))
    for o in range(NY):
        for c in range(2):
            if o > 0:
                push(gbuf.at[tp], gbuf.at[tp], ("gain", 0), dev(dy=o, c=c), tp)
    push(gbuf.at[tp], gbuf.at[tp], ("gain", 0), dev(c=other), tp)
    for k, (s, d) in enumerate(weights):
        if k >= 4:
            push(s, d, ("w", k), dev(c=other))

    def bslice(ref, p, h, r):
        if h == 0:
            return ref.at[h, p, 0:BLK, r * HALF : (r + 1) * HALF]
        return ref.at[h, p, r * BLK : (r + 1) * BLK, 0:HALF]

    def cslice(ref, p, h, r):
        if h == 0:
            return ref.at[h, p, r * BLK : (r + 1) * BLK, :]
        return ref.at[h, p, :, r * HALF : (r + 1) * HALF]

    def along(stage, h, step):
        on_y = (stage == "b") == (h == 0)
        return dev(dy=step % NY) if on_y else dev(dx=step % NX)

    def ring_first(view, stage, key, p, h, ref):
        push(view(ref, p, h, 0), view(ref, p, h, 3), (key, p, h, 3), along(stage, h, 1))
        push(view(ref, p, h, 0), view(ref, p, h, 1), (key, p, h, 1), along(stage, h, -1))

    def ring_forward(view, stage, key, p, h, ref):
        near, step = (3, 1) if p % 2 == 0 else (1, -1)
        arrive(view(ref, p, h, near), (key, p, h, near))
        push(view(ref, p, h, near), view(ref, p, h, 2), (key, p, h, 2), along(stage, h, step))
        arrive(view(ref, p, h, 4 - near), (key, p, h, 4 - near))

    def rslice(p, r):
        return rbuf.at[p, r * BLK : (r + 1) * BLK, :]

    def stage_a(p):
        for h in range(2):
            if p > 0:
                arrive(hbuf.at[h, p, 0:BLK, 0:HALF], ("z", p, h))
        if p == 0:
            arrive(hbuf.at[other, 0, 0:BLK, 0:HALF], ("z", 0, 0), other)
        else:
            arrive(rslice(p, 0), ("zr", p))
        for h in range(2):
            ring_first(bslice, "b", "ab", p, h, hbuf)
        push(rslice(p, 0), rslice(p, 3), ("br", p, 3), dev(dx=1))
        push(rslice(p, 0), rslice(p, 1), ("br", p, 1), dev(dx=3))

    def stage_b(p):
        for h in range(2):
            ring_forward(bslice, "b", "ab", p, h, hbuf)
        near, step = (3, 1) if p % 2 == 0 else (1, 3)
        arrive(rslice(p, near), ("br", p, near))
        push(rslice(p, near), rslice(p, 2), ("br", p, 2), dev(dx=step))
        arrive(rslice(p, 4 - near), ("br", p, 4 - near))

    def stage_c(p):
        for h in range(2):
            arrive(bslice(hbuf, p, h, 2), ("ab", p, h, 2))
            ring_first(cslice, "c", "ac", p, h, hbuf)
        arrive(rslice(p, 2), ("br", p, 2))

    def stage_d(p):
        for h in range(2):
            ring_forward(cslice, "c", "ac", p, h, hbuf)

    def stage_e(p):
        for h in range(2):
            arrive(cslice(hbuf, p, h, 2), ("ac", p, h, 2))

    def weight_ready(ks):
        for k in ks:
            local[k].wait()
            arrive(partner[k], ("w", k))

    def plan_partner():
        def lo(first):
            return pl.ds(pl.multiple_of(first + other * 128, 128), 128)

        out = []
        for e in range(2):
            out += [wgu.at[:, lo(e * 256)], wgu.at[:, lo(512 + e * 256)]]
        out += [wsgu.at[:, lo(0)], wsgu.at[:, lo(256)]]
        out += [wd.at[lo(e * 256), :] for e in range(2)]
        return out + [wsd.at[lo(0), :]]

    partner = plan_partner()

    def dot(a, b):
        return jnp.dot(a, b, preferred_element_type=F32)

    def columns(h, r):
        return pl.ds(pl.multiple_of(((y + r) % NY) * 1024 + h * HALF, HALF), HALF)

    def silu(v):
        return v / (1.0 + jnp.exp(-v))

    def compute(g, planes):
        first = g * planes
        rows = planes * 64
        if g == 0:
            for o in range(NY):
                for c in range(2):
                    if o > 0:
                        k = ((y + o) % NY) * 2 + c
                        arrive(gbuf.at[k], ("gain", 0), k)
            k = y * 2 + other
            arrive(gbuf.at[k], ("gain", 0), k)

        def normalise(b, carry):
            p = first + b // 4
            at = pl.ds(pl.multiple_of((b % 4) * BLK, BLK), BLK)
            to = pl.ds(pl.multiple_of(b * BLK, BLK), BLK)
            squares = jnp.zeros((BLK, HALF), F32)
            for h in range(2):
                for r in range(NY):
                    v = hbuf[h, p, at, r * HALF : (r + 1) * HALF].astype(F32)
                    squares = squares + v * v
            scale = lax.rsqrt(jnp.sum(squares, axis=1, keepdims=True) / 4096.0 + EPS)
            for h in range(2):
                for r in range(NY):
                    v = hbuf[h, p, at, r * HALF : (r + 1) * HALF].astype(F32)
                    gain = gbuf[((y + r) % NY) * 2 + h]
                    hn[to, columns(h, r)] = (v * scale * gain).astype(BF16)
            return carry

        lax.fori_loop(0, rows // BLK, normalise, 0)
        if g == 0:
            weight_ready(range(0, 4))
        route = rbuf[first : first + planes].reshape(rows, 128)
        pick_row = lax.broadcasted_iota(jnp.int32, (128, 256), 0) % 64
        for e in range(2):
            pick = jnp.where(pick_row == ep * 2 + e, 1.0, 0.0).astype(BF16)
            share = dot(route, pick)
            gate = dot(hn[...], wgu[:, e * 256 : (e + 1) * 256])
            up = dot(hn[...], wgu[:, 512 + e * 256 : 768 + e * 256])
            inner[:, e * 256 : (e + 1) * 256] = (silu(gate) * up * share).astype(BF16)
        if g == 0:
            weight_ready(range(4, 9))
            own = hn[0:BLK, :]
            shared = (silu(dot(own, wsgu[:, 0:256])) * dot(own, wsgu[:, 256:512])).astype(BF16)
        for h in range(2):
            for r in range(NY):
                part = dot(inner[...], wd[:, columns(h, r)])
                cols = slice(r * HALF, (r + 1) * HALF)
                pbuf[h, first : first + planes, :, cols] = part.reshape(planes, 64, HALF).astype(BF16)
                if g == 0:
                    extra = dot(shared, wsd[:, columns(h, r)])
                    pbuf[h, 0, 0:BLK, cols] = (part[0:BLK] + extra).astype(BF16)

    def land(stage, p, h, r):
        if stage == "b":
            return fb.at[h, p, r - 1]
        return (fc0 if h == 0 else fc1).at[p, r - 1]

    def sum_first(view, stage, key, p, h):
        near, step = (1, 1) if p % 2 == 0 else (3, -1)
        push(view(pbuf, p, h, 2), land(stage, p, h, 2), (key, p, h, 2), along(stage, h, step))
        push(view(pbuf, p, h, 4 - near), land(stage, p, h, near), (key, p, h, near), along(stage, h, -step))

    def sum_forward(view, stage, key, p, h):
        near, step = (1, 1) if p % 2 == 0 else (3, -1)
        arrive(land(stage, p, h, 2), (key, p, h, 2))
        mine = view(pbuf, p, h, near)
        mine[...] = (mine[...].astype(F32) + land(stage, p, h, 2)[...].astype(F32)).astype(BF16)
        push(mine, land(stage, p, h, 4 - near), (key, p, h, 4 - near), along(stage, h, step))

    def sum_last(view, stage, key, p, h):
        for r in (1, 3):
            arrive(land(stage, p, h, r), (key, p, h, r))
        mine = view(pbuf, p, h, 0)
        mine[...] = (
            mine[...].astype(F32) + land(stage, p, h, 1)[...].astype(F32) + land(stage, p, h, 3)[...].astype(F32)
        ).astype(BF16)

    def stage_r1(p):
        for h in range(2):
            sum_first(cslice, "c", "rc", p, h)

    def stage_r2(p):
        for h in range(2):
            sum_forward(cslice, "c", "rc", p, h)

    def stage_r3(p):
        for h in range(2):
            sum_last(cslice, "c", "rc", p, h)
            sum_first(bslice, "b", "rb", p, h)

    def stage_r4(p):
        for h in range(2):
            sum_forward(bslice, "b", "rb", p, h)

    def stage_r5(p):
        for h in range(2):
            sum_last(bslice, "b", "rb", p, h)
        dz = SEQ[p]
        q = POS[(-dz) % NZ]
        if p == 0:
            zb[0, core] = pbuf[core, 0, 0:BLK, 0:HALF]
            push(pbuf.at[other, 0, 0:BLK, 0:HALF], zb.at[0, core], ("rz", 0, 0), dev(c=other), core)
        else:
            for h in range(2):
                push(pbuf.at[h, p, 0:BLK, 0:HALF], zb.at[q, core], ("rz", q, 0), dev(dz=dz, c=h), core)

    planes = 2
    stages = (stage_a, stage_b, stage_c, stage_d, stage_e)
    back = (stage_r2, stage_r3, stage_r4, stage_r5)
    ready = {}
    for tick in range(NZ + 4 + len(back)):
        for k in range(len(back) - 1, -1, -1):
            for p in range(NZ):
                if ready.get(p) == tick - 1 - k:
                    back[k](p)
        for k in range(4, -1, -1):
            if 0 <= tick - k < NZ:
                stages[k](tick - k)
        last = tick - 4
        if 0 <= last < NZ and (last + 1) % planes == 0:
            g = last // planes
            compute(g, planes)
            for p in range(g * planes, (g + 1) * planes):
                stage_r1(p)
                ready[p] = tick

    for p in range(1, NZ):
        for c in range(2):
            arrive(zb.at[p, c], ("rz", p, c))
    arrive(zb.at[0, other], ("rz", 0, 0), other)
    for c in range(2):
        total = zb[0, c].astype(F32)
        for p in range(1, NZ):
            total = total + zb[p, c].astype(F32)
        alive = live[c * BLK : (c + 1) * BLK, 0:1]
        out_ref[c] = jnp.where(alive, total, 0.0).astype(BF16)
    for cp in started:
        cp.wait_send()


def body(hidden, norm_gain, expert_ids, route_weights, lengths, gate_proj, up_proj, down_proj, sgate, sup, sdown):
    vmem = pl.BlockSpec(memory_space=pltpu.VMEM)
    anywhere = pl.BlockSpec(memory_space=pl.ANY)
    n = IDS.count
    out = pl.pallas_call(
        kernel,
        out_shape=jax.ShapeDtypeStruct((2, BLK, HALF), BF16),
        in_specs=[vmem] * 4 + [pl.BlockSpec(memory_space=pltpu.SMEM)] + [anywhere] * 6,
        out_specs=vmem,
        scratch_shapes=[
            pltpu.VMEM((2, NZ, 64, 2048), BF16),
            pltpu.VMEM((2, NZ, 64, 2048), BF16),
            pltpu.VMEM((NZ, 64, 128), BF16),
            pltpu.VMEM((2, BLK, 128), BF16),
            pltpu.VMEM((8, 1, HALF), F32),
            pltpu.VMEM((128, 4096), BF16),
            pltpu.VMEM((128, 512), BF16),
            pltpu.VMEM((4096, 1024), BF16),
            pltpu.VMEM((512, 4096), BF16),
            pltpu.VMEM((4096, 512), BF16),
            pltpu.VMEM((256, 4096), BF16),
            pltpu.VMEM((NZ, 3, BLK, 2048), BF16),
            pltpu.VMEM((NZ, 3, 64, HALF), BF16),
            pltpu.VMEM((2, NZ, 3, BLK, HALF), BF16),
            pltpu.VMEM((NZ, 2, BLK, HALF), BF16),
            pltpu.SemaphoreType.DMA((9,)),
            pltpu.SemaphoreType.DMA((n,)),
            pltpu.SemaphoreType.DMA((n,)),
        ],
        compiler_params=pltpu.CompilerParams(
            collective_id=0, has_side_effects=True, vmem_limit_bytes=60 * 1024 * 1024
        ),
    )(
        hidden.reshape(2, BLK, HALF),
        norm_gain.reshape(1, HALF),
        expert_ids,
        route_weights,
        lengths,
        gate_proj,
        up_proj,
        down_proj,
        sgate,
        sup,
        sdown,
    )
    return out.reshape(2 * BLK, HALF)


def solution(mesh):
    placed = (
        P("ep", "tp"),
        P("tp"),
        P("ep", None),
        P("ep", None),
        P("ep"),
        P("ep", None, "tp"),
        P("ep", None, "tp"),
        P("ep", "tp", None),
        P(None, "tp"),
        P(None, "tp"),
        P("tp", None),
    )
    return jax.shard_map(body, mesh=mesh, in_specs=placed, out_specs=P("ep", "tp"), check_vma=False)
```

```python
import functools

import jax
import jax.numpy as jnp
from jax import lax
from jax.experimental import pallas as pl
from jax.experimental.pallas import tpu as pltpu
from jax.sharding import PartitionSpec as P

MESH = pl.DeviceIdType.MESH
EPS = 1e-06
NZ, NX, NY = 8, 4, 4
BLK = 16
HALF = 512
F32, BF16 = jnp.float32, jnp.bfloat16
SEQ = (0, 1, 7, 2, 6, 3, 5, 4)
POS = {dz: i for i, dz in enumerate(SEQ)}


GROUPS_OF = ((0, 1), (2, 3), (4, 5), (6, 7))
ORDER = (
    "a00", "a01", "i0", "a11", "a10", "i1", "b00", "b01", "j0", "a20", "a21", "i2", "a30", "a31", "i3", "b11",
    "b10", "j1", "a50", "i5", "a40", "a51", "a41", "i4", "c00", "c01", "k0", "b20", "b21", "j2", "a61", "i6",
    "a60", "b30", "a71", "a70", "i7", "j3", "b31", "c10", "c11", "k1", "j5", "b50", "b40", "b41", "b51", "j4",
    "d01", "d00", "c20", "c21", "k2", "b60", "c30", "b61", "j6", "b70", "b71", "j7", "k3", "c31", "d11", "c40",
    "c50", "c41", "d10", "k4", "k5", "c51", "e01", "e00", "c70", "d21", "c60", "d20", "d31", "d30", "c71", "k7",
    "e11", "c61", "k6", "d41", "d40", "d50", "d51", "e10", "n0", "m0", "d70", "v01", "d71", "d60", "v00", "r10",
    "d61", "r00", "r01", "r11", "e31", "e21", "e20", "e30", "n1", "m1", "v10", "e51", "r30", "e40", "e60", "r20",
    "e50", "v11", "r31", "r21", "e70", "e71", "e61", "n3", "m3", "v31", "r61", "v30", "r71", "r70", "r60", "e41",
    "n2", "m2", "v21", "r41", "v20", "r40", "r51", "s31", "s11", "s21", "s20", "r50", "s10", "s30", "s61", "s01",
    "s00", "s70", "s71", "s60", "s41", "s40", "s51", "t20", "s50", "t31", "t21", "t10", "t61", "t11", "t30", "t00",
    "t71", "t01", "t70", "t60", "t51", "t41", "u20", "t50", "t40", "u10", "u31", "u30", "u21", "u00", "u61", "u11",
    "u70", "u71", "u60", "u01", "u51", "w20", "u41", "u50", "w31", "u40", "w21", "w10", "w00", "w61", "w30", "w11",
    "w70", "w71", "w60", "w01", "w51", "w41", "w50", "w40",
)
LAST_HALF = 1 if ORDER.index("w00") < ORDER.index("w01") else 0


class Ids:
    def __init__(self):
        self.table, self.count = {}, 0

    def at(self, *key):
        if key not in self.table:
            self.table[key] = self.count
            self.count += 1
        return self.table[key]


def build_ids():
    ids = Ids()
    for key in ("zp", "rzp"):
        ids.count = ids.at(key) + 2
    for p in range(NZ):
        for h in range(2):
            ids.at("z", p, h)
    for p in range(NZ):
        ids.at("zr", p)
        for r in (1, 2, 3):
            ids.at("br", p, r)
            for h in range(2):
                for stage in ("ab", "ac", "rc", "rb"):
                    ids.at(stage, p, h, r)
        for c in range(2):
            ids.at("rz", p, c)
    for k in range(8):
        ids.at("gain", k)
    for k in range(9):
        ids.at("w", k)
    return ids


IDS = build_ids()
RINGS = ("ab", "ac", "rb", "rc")
GROUPS = [k + str(h) for k in RINGS for h in range(2)] + ["z", "zp", "zr", "br", "gain", "rz", "rzp", "w"]


def kernel(
    hidden_ref, gain_ref, eid_ref, rw_ref, len_ref, gate_ref, up_ref, down_ref, sgate_ref, sup_ref, sdown_ref,
    out_ref,
    hbuf, pbuf, rbuf, rown, gbuf, hn, inner, shared, wgu, wd, wsgu, wsd, fc0, fc1, fb, zb, lsem, wsem, ssem, rsem,
):
    ep, tp = lax.axis_index("ep"), lax.axis_index("tp")
    z, x = ep // NX, ep % NX
    y, core = tp // 2, tp % 2
    other = 1 - core

    def dev(dz=0, dx=0, dy=0, c=None):
        c = core if c is None else c
        return (((z + dz) % NZ) * NX + (x + dx) % NX, ((y + dy) % NY) * 2 + c)

    def group(key):
        return GROUPS.index(key[0] + str(key[2]) if key[0] in RINGS else key[0])

    def push(src, dst, key, to, add=0):
        i = IDS.at(*key) + add
        sem = ssem.at[group(key)]
        if key[0] == "w":
            sem = wsem.at[key[1]]
        pltpu.make_async_remote_copy(
            src_ref=src, dst_ref=dst, send_sem=sem, recv_sem=rsem.at[i], device_id=to, device_id_type=MESH
        ).start()

    def sent(ref, sem):
        pltpu.make_async_remote_copy(
            src_ref=ref, dst_ref=ref, send_sem=sem, recv_sem=rsem.at[0], device_id=dev(c=other), device_id_type=MESH
        ).wait_send()

    def arrive(dst, key, add=0):
        i = IDS.at(*key) + add
        pltpu.make_async_remote_copy(
            src_ref=dst, dst_ref=dst, send_sem=ssem.at[0], recv_sem=rsem.at[i], device_id=dev(c=other), device_id_type=MESH
        ).wait_recv()

    def lanes(first):
        return pl.ds(pl.multiple_of(first + core * 128, 128), 128)

    weights = []
    for e in range(2):
        weights.append((gate_ref.at[e], wgu.at[:, lanes(e * 256)]))
        weights.append((up_ref.at[e], wgu.at[:, lanes(512 + e * 256)]))
    weights.append((sgate_ref, wsgu.at[:, lanes(0)]))
    weights.append((sup_ref, wsgu.at[:, lanes(256)]))
    for e in range(2):
        weights.append((down_ref.at[e], wd.at[lanes(e * 256), :]))
    weights.append((sdown_ref, wsd.at[lanes(0), :]))
    local = [pltpu.make_async_copy(s, d, lsem.at[k]) for k, (s, d) in enumerate(weights)]
    for cp in local:
        cp.start()

    barrier = pltpu.get_barrier_semaphore()
    peers = [dev(dz=o, c=c) for o in range(1, NZ) for c in range(2)] + [dev(c=other)]
    peers += [dev(dy=o, c=c) for o in range(1, NY) for c in range(2)]
    peers += [dev(dx=1), dev(dx=-1 + NX)]
    for peer in peers:
        pl.semaphore_signal(barrier, inc=1, device_id=peer, device_id_type=MESH)

    def live_slots(shape, dim):
        slot = lax.broadcasted_iota(jnp.int32, shape, dim)
        seq_len = jnp.zeros(shape, jnp.int32)
        for q in range(4):
            seq_len = jnp.where(slot // 8 == q, len_ref[q], seq_len)
        return slot % 8 < seq_len

    expert = lax.broadcasted_iota(jnp.int32, (128, 32), 0)
    mix = jnp.zeros((128, 32), F32)
    for k in range(8):
        mix = mix + jnp.where(eid_ref[k : k + 1, :] == expert % 64, rw_ref[k : k + 1, :], 0.0)
    mix = jnp.where(live_slots((128, 32), 1), mix, 0.0)
    high = mix.astype(BF16).astype(F32)
    terms = jnp.where(expert < 64, high, mix - high).T
    rown[...] = terms.reshape(2, BLK, 128).astype(BF16)
    rbuf[0, 0:BLK, :] = rown[core]
    gbuf[tp] = gain_ref[...]
    hbuf[core, 0, 0:BLK, 0:HALF] = hidden_ref[core]

    with jax.named_scope("barrier"):
        pl.semaphore_wait(barrier, len(peers))

    for o in (1, 7, 2, 6, 3, 5, 4):
        p = POS[(-o) % NZ]
        if o == 1:
            push(hidden_ref.at[other], hbuf.at[core, 0, 0:BLK, 0:HALF], ("zp",), dev(c=other), core)
        for c in range(2):
            push(hidden_ref.at[c], hbuf.at[core, p, 0:BLK, 0:HALF], ("z", p, 0), dev(dz=o, c=c), core)
        push(rown.at[core], rbuf.at[p, 0:BLK, :], ("zr", p), dev(dz=o))
    for k, (s, d) in enumerate(weights):
        if k < 4:
            push(s, d, ("w", k), dev(c=other))
    for o in range(NY):
        for c in range(2):
            if o > 0:
                push(gbuf.at[tp], gbuf.at[tp], ("gain", 0), dev(dy=o, c=c), tp)
    push(gbuf.at[tp], gbuf.at[tp], ("gain", 0), dev(c=other), tp)
    for k, (s, d) in enumerate(weights):
        if k >= 4:
            push(s, d, ("w", k), dev(c=other))

    def bslice(ref, p, h, r):
        if h == 0:
            return ref.at[h, p, 0:BLK, r * HALF : (r + 1) * HALF]
        return ref.at[h, p, r * BLK : (r + 1) * BLK, 0:HALF]

    def cslice(ref, p, h, r):
        if h == 0:
            return ref.at[h, p, r * BLK : (r + 1) * BLK, :]
        return ref.at[h, p, :, r * HALF : (r + 1) * HALF]

    def along(stage, h, step):
        on_y = (stage == "b") == (h == 0)
        return dev(dy=step % NY) if on_y else dev(dx=step % NX)

    def ring_first(view, stage, key, p, h, ref):
        push(view(ref, p, h, 0), view(ref, p, h, 3), (key, p, h, 3), along(stage, h, 1))
        push(view(ref, p, h, 0), view(ref, p, h, 1), (key, p, h, 1), along(stage, h, -1))

    def ring_forward(view, stage, key, p, h, ref):
        near, step = (3, 1) if p % 2 == 0 else (1, -1)
        arrive(view(ref, p, h, near), (key, p, h, near))
        push(view(ref, p, h, near), view(ref, p, h, 2), (key, p, h, 2), along(stage, h, step))

    def ring_done(view, key, p, h, ref):
        near = 3 if p % 2 == 0 else 1
        arrive(view(ref, p, h, 4 - near), (key, p, h, 4 - near))
        arrive(view(ref, p, h, 2), (key, p, h, 2))

    def rslice(p, r):
        return rbuf.at[p, r * BLK : (r + 1) * BLK, :]

    def route_a(p):
        if p > 0:
            arrive(rslice(p, 0), ("zr", p))
        push(rslice(p, 0), rslice(p, 3), ("br", p, 3), dev(dx=1))
        push(rslice(p, 0), rslice(p, 1), ("br", p, 1), dev(dx=3))

    def route_b(p):
        near, step = (3, 1) if p % 2 == 0 else (1, 3)
        arrive(rslice(p, near), ("br", p, near))
        push(rslice(p, near), rslice(p, 2), ("br", p, 2), dev(dx=step))

    def route_c(p):
        near = 3 if p % 2 == 0 else 1
        arrive(rslice(p, 4 - near), ("br", p, 4 - near))
        arrive(rslice(p, 2), ("br", p, 2))

    def gather_a(p, h):
        if p > 0:
            arrive(hbuf.at[h, p, 0:BLK, 0:HALF], ("z", p, h))
        elif h == 0:
            arrive(hbuf.at[other, 0, 0:BLK, 0:HALF], ("zp",), other)
        ring_first(bslice, "b", "ab", p, h, hbuf)

    def gather_b(p, h):
        ring_forward(bslice, "b", "ab", p, h, hbuf)

    def gather_c(p, h):
        ring_done(bslice, "ab", p, h, hbuf)
        ring_first(cslice, "c", "ac", p, h, hbuf)

    def gather_d(p, h):
        ring_forward(cslice, "c", "ac", p, h, hbuf)

    def gather_e(p, h):
        ring_done(cslice, "ac", p, h, hbuf)

    def weight_ready(ks):
        for k in ks:
            local[k].wait()
            arrive(partner[k], ("w", k))

    def plan_partner():
        def lo(first):
            return pl.ds(pl.multiple_of(first + other * 128, 128), 128)

        out = []
        for e in range(2):
            out += [wgu.at[:, lo(e * 256)], wgu.at[:, lo(512 + e * 256)]]
        out += [wsgu.at[:, lo(0)], wsgu.at[:, lo(256)]]
        out += [wd.at[lo(e * 256), :] for e in range(2)]
        return out + [wsd.at[lo(0), :]]

    partner = plan_partner()

    def dot(a, b):
        return jnp.dot(a, b, preferred_element_type=F32)

    def columns(h, r):
        return pl.ds(pl.multiple_of(((y + r) % NY) * 1024 + h * HALF, HALF), HALF)

    def silu(v):
        return v / (1.0 + jnp.exp(-v))

    def normalise(g):
        first, planes = GROUPS_OF[g][0], len(GROUPS_OF[g])
        if g == 0:
            for o in range(NY):
                for c in range(2):
                    if o > 0:
                        k = ((y + o) % NY) * 2 + c
                        arrive(gbuf.at[k], ("gain", 0), k)
            k = y * 2 + other
            arrive(gbuf.at[k], ("gain", 0), k)

        def block(b, carry):
            p = first + b // 4
            at = pl.ds(pl.multiple_of((b % 4) * BLK, BLK), BLK)
            to = pl.ds(pl.multiple_of(b * BLK, BLK), BLK)
            squares = jnp.zeros((BLK, HALF), F32)
            for h in range(2):
                for r in range(NY):
                    v = hbuf[h, p, at, r * HALF : (r + 1) * HALF].astype(F32)
                    squares = squares + v * v
            scale = lax.rsqrt(jnp.sum(squares, axis=1, keepdims=True) / 4096.0 + EPS)
            for h in range(2):
                for r in range(NY):
                    v = hbuf[h, p, at, r * HALF : (r + 1) * HALF].astype(F32)
                    gain = gbuf[((y + r) % NY) * 2 + h]
                    hn[to, columns(h, r)] = (v * scale * gain).astype(BF16)
            return carry

        lax.fori_loop(0, planes * 4, block, 0)

    def hidden_units(g):
        first, planes = GROUPS_OF[g][0], len(GROUPS_OF[g])
        rows = planes * 64
        if g == 0:
            weight_ready(range(0, 4))
        route = rbuf[first : first + planes].reshape(rows, 128)
        pick_row = lax.broadcasted_iota(jnp.int32, (128, 256), 0) % 64
        for e in range(2):
            pick = jnp.where(pick_row == ep * 2 + e, 1.0, 0.0).astype(BF16)
            share = dot(route, pick)
            gate = dot(hn[0:rows, :], wgu[:, e * 256 : (e + 1) * 256])
            up = dot(hn[0:rows, :], wgu[:, 512 + e * 256 : 768 + e * 256])
            inner[0:rows, e * 256 : (e + 1) * 256] = (silu(gate) * up * share).astype(BF16)
        if g == 0:
            weight_ready(range(4, 9))
            own = hn[0:BLK, :]
            shared[...] = (silu(dot(own, wsgu[:, 0:256])) * dot(own, wsgu[:, 256:512])).astype(BF16)

    def outputs(g, h):
        first, planes = GROUPS_OF[g][0], len(GROUPS_OF[g])
        rows = planes * 64
        for r in range(NY):
            part = dot(inner[0:rows, :], wd[:, columns(h, r)])
            cols = slice(r * HALF, (r + 1) * HALF)
            pbuf[h, first : first + planes, :, cols] = part.reshape(planes, 64, HALF).astype(BF16)
            if g == 0:
                extra = dot(shared[...], wsd[:, columns(h, r)])
                pbuf[h, 0, 0:BLK, cols] = (part[0:BLK] + extra).astype(BF16)

    def land(stage, p, h, r):
        if stage == "b":
            return fb.at[h, p, r - 1]
        return (fc0 if h == 0 else fc1).at[p, r - 1]

    def sum_first(view, stage, key, p, h):
        near, step = (1, 1) if p % 2 == 0 else (3, -1)
        push(view(pbuf, p, h, 2), land(stage, p, h, 2), (key, p, h, 2), along(stage, h, step))
        push(view(pbuf, p, h, 4 - near), land(stage, p, h, near), (key, p, h, near), along(stage, h, -step))

    def sum_forward(view, stage, key, p, h):
        near, step = (1, 1) if p % 2 == 0 else (3, -1)
        arrive(land(stage, p, h, 2), (key, p, h, 2))
        mine = view(pbuf, p, h, near)
        mine[...] = (mine[...].astype(F32) + land(stage, p, h, 2)[...].astype(F32)).astype(BF16)
        push(mine, land(stage, p, h, 4 - near), (key, p, h, 4 - near), along(stage, h, step))

    def sum_last(view, stage, key, p, h):
        for r in (1, 3):
            arrive(land(stage, p, h, r), (key, p, h, r))
        mine = view(pbuf, p, h, 0)
        mine[...] = (
            mine[...].astype(F32) + land(stage, p, h, 1)[...].astype(F32) + land(stage, p, h, 3)[...].astype(F32)
        ).astype(BF16)

    def sum_r(p, h):
        sum_first(cslice, "c", "rc", p, h)

    def sum_s(p, h):
        sum_forward(cslice, "c", "rc", p, h)

    def sum_t(p, h):
        sum_last(cslice, "c", "rc", p, h)
        sum_first(bslice, "b", "rb", p, h)

    def sum_u(p, h):
        sum_forward(bslice, "b", "rb", p, h)

    def sum_w(p, h):
        sum_last(bslice, "b", "rb", p, h)
        dz = SEQ[p]
        q = POS[(-dz) % NZ]
        if p > 0:
            push(pbuf.at[h, p, 0:BLK, 0:HALF], zb.at[q, core], ("rz", q, 0), dev(dz=dz, c=h), core)
        elif h == LAST_HALF:
            zb[0, core] = pbuf[core, 0, 0:BLK, 0:HALF]
            push(pbuf.at[other, 0, 0:BLK, 0:HALF], zb.at[0, core], ("rzp",), dev(c=other), core)

    steps = dict(i=route_a, j=route_b, k=route_c, a=gather_a, b=gather_b, c=gather_c, d=gather_d, e=gather_e)
    steps |= dict(n=normalise, m=hidden_units, v=outputs, r=sum_r, s=sum_s, t=sum_t, u=sum_u, w=sum_w)
    for name in ORDER:
        with jax.named_scope(name):
            steps[name[0]](*[int(digit) for digit in name[1:]])

    with jax.named_scope("final"):
        for p in range(1, NZ):
            for c in range(2):
                arrive(zb.at[p, c], ("rz", p, c))
        arrive(zb.at[0, other], ("rzp",), other)
    live = live_slots((2 * BLK, HALF), 0)
    for c in range(2):
        total = zb[0, c].astype(F32)
        for p in range(1, NZ):
            total = total + zb[p, c].astype(F32)
        alive = live[c * BLK : (c + 1) * BLK]
        out_ref[c] = jnp.where(alive, total, 0.0).astype(BF16)
    with jax.named_scope("drain"):
        rings = {"ab0": fb.at[0], "ab1": fb.at[1], "ac0": fc0, "ac1": fc1}
        rings |= {"rb0": fb.at[0], "rb1": fb.at[1], "rc0": fc0, "rc1": fc1}
        rings |= {"z": zb.at[1:NZ], "zp": zb.at[0, 0], "rz": zb.at[1:NZ], "rzp": zb.at[0, 0]}
        rings |= {"zr": rbuf.at[0:7, 0:BLK, :], "br": rbuf.at[:, 0:48, :], "gain": gbuf.at[0:7]}
        for name, ref in rings.items():
            sent(ref, ssem.at[GROUPS.index(name)])
        for k, (s, _) in enumerate(weights):
            sent(s, wsem.at[k])


def body(hidden, norm_gain, expert_ids, route_weights, lengths, gate_proj, up_proj, down_proj, sgate, sup, sdown):
    vmem = pl.BlockSpec(memory_space=pltpu.VMEM)
    anywhere = pl.BlockSpec(memory_space=pl.ANY)
    n = IDS.count
    out = pl.pallas_call(
        kernel,
        out_shape=jax.ShapeDtypeStruct((2, BLK, HALF), BF16),
        in_specs=[vmem] * 4 + [pl.BlockSpec(memory_space=pltpu.SMEM)] + [anywhere] * 6,
        out_specs=vmem,
        scratch_shapes=[
            pltpu.VMEM((2, NZ, 64, 2048), BF16),
            pltpu.VMEM((2, NZ, 64, 2048), BF16),
            pltpu.VMEM((NZ, 64, 128), BF16),
            pltpu.VMEM((2, BLK, 128), BF16),
            pltpu.VMEM((8, 1, HALF), F32),
            pltpu.VMEM((128, 4096), BF16),
            pltpu.VMEM((128, 512), BF16),
            pltpu.VMEM((BLK, 256), BF16),
            pltpu.VMEM((4096, 1024), BF16),
            pltpu.VMEM((512, 4096), BF16),
            pltpu.VMEM((4096, 512), BF16),
            pltpu.VMEM((256, 4096), BF16),
            pltpu.VMEM((NZ, 3, BLK, 2048), BF16),
            pltpu.VMEM((NZ, 3, 64, HALF), BF16),
            pltpu.VMEM((2, NZ, 3, BLK, HALF), BF16),
            pltpu.VMEM((NZ, 2, BLK, HALF), BF16),
            pltpu.SemaphoreType.DMA((9,)),
            pltpu.SemaphoreType.DMA((9,)),
            pltpu.SemaphoreType.DMA((len(GROUPS),)),
            pltpu.SemaphoreType.DMA((n,)),
        ],
        compiler_params=pltpu.CompilerParams(
            collective_id=0, has_side_effects=True, vmem_limit_bytes=60 * 1024 * 1024
        ),
    )(
        hidden.reshape(2, BLK, HALF),
        norm_gain.reshape(1, HALF),
        expert_ids.T,
        route_weights.T,
        lengths,
        gate_proj,
        up_proj,
        down_proj,
        sgate,
        sup,
        sdown,
    )
    return out.reshape(2 * BLK, HALF)


def solution(mesh):
    placed = (
        P("ep", "tp"),
        P("tp"),
        P("ep", None),
        P("ep", None),
        P("ep"),
        P("ep", None, "tp"),
        P("ep", None, "tp"),
        P("ep", "tp", None),
        P(None, "tp"),
        P(None, "tp"),
        P("tp", None),
    )
    return jax.shard_map(body, mesh=mesh, in_specs=placed, out_specs=P("ep", "tp"), check_vma=False)
```

```python
import functools

import jax
import jax.numpy as jnp
from jax import lax
from jax.experimental import pallas as pl
from jax.experimental.pallas import tpu as pltpu
from jax.sharding import PartitionSpec as P

MESH = pl.DeviceIdType.MESH
EPS = 1e-06
NZ, NX, NY = 8, 4, 4
BLK = 16
HALF = 512
F32, BF16 = jnp.float32, jnp.bfloat16
SEQ = (0, 1, 7, 2, 6, 3, 5, 4)
POS = {dz: i for i, dz in enumerate(SEQ)}


GROUPS_OF = ((0, 3), (4, 5), (1, 2), (6, 7))
ORDER = (
    "i0", "a00", "a01", "j0", "i1", "b00", "b01", "i2", "c00", "c01", "k0", "a31", "a30", "i3", "j1", "a40",
    "a41", "a50", "a51", "i4", "i5", "j2", "i6", "a61", "a60", "d00", "a71", "d01", "a70", "i7", "b31", "b30",
    "j3", "k1", "b50", "b51", "j5", "b40", "b41", "c31", "c30", "j4", "k2", "b60", "j6", "c40", "c41", "b71",
    "b70", "j7", "b61", "k3", "c50", "e01", "c51", "k5", "e00", "d31", "d30", "c60", "k4", "k6", "c70", "d41",
    "c71", "k7", "d40", "c61", "d51", "d50", "e11", "e21", "e31", "e30", "n0", "m0", "v01", "r31", "v00", "r30",
    "e20", "d60", "d71", "e10", "e41", "e40", "d70", "n2", "e50", "d61", "m2", "v20", "v21", "e51", "n1", "s31",
    "s30", "m1", "v10", "r40", "v11", "r41", "r51", "r50", "e70", "e61", "e71", "e60", "n3", "m3", "t30", "t31",
    "v30", "r60", "r70", "v31", "r71", "s40", "r61", "q03", "q01", "s41", "q02", "r00", "q00", "s50", "s51", "q12",
    "u31", "w31", "u30", "w30", "q13", "r01", "s71", "s60", "q11", "s70", "s61", "q10", "t51", "t40", "t41", "t50",
    "s00", "s01", "t70", "t71", "t60", "t61", "u51", "w51", "u40", "w40", "u41", "w41", "u50", "w50", "t00", "t01",
    "u71", "w71", "u70", "w70", "u61", "w61", "u60", "w60", "u00", "w00", "u01", "w01",
)
RELAYED = (1, 2)
DIRECT_OUT = (0, 3, 4)
DIRECT_BACK = (0, 3, 4, 5, 6, 7)
PLANES = tuple(p for p in range(8) if p not in RELAYED)
FIRST_HALF = 0 if ORDER.index("a00") < ORDER.index("a01") else 1
LAST_HALF = 1 if ORDER.index("w00") < ORDER.index("w01") else 0


def shared_key(key):
    if key[0] in ("ab", "ac"):
        return key if key[3] == (3 if key[1] % 2 == 0 else 1) else key[:3] + (2,)
    if key[0] in ("rb", "rc"):
        direct = key[0] == "rb" and key[1] in DIRECT_BACK
        return key[:3] + (1,) if direct or key[3] != 2 else key
    if key[0] == "br":
        return key if key[2] == (3 if key[1] % 2 == 0 else 1) else key[:2] + (2,)
    if key[0] == "rz":
        return ("rz",)
    return key


class Ids:
    def __init__(self):
        self.table, self.count = {}, 0

    def at(self, *key):
        key = shared_key(key)
        if key not in self.table:
            self.table[key] = self.count
            self.count += 1
        return self.table[key]


def build_ids():
    ids = Ids()
    ids.count = ids.at("zp") + 2
    for p in range(NZ):
        for h in range(2):
            ids.at("z", p, h)
    for p in range(NZ):
        ids.at("zr", p)
        for r in (1, 2, 3):
            ids.at("br", p, r)
            for h in range(2):
                for stage in ("ab", "ac", "rc", "rb"):
                    ids.at(stage, p, h, r)
    for name in ("rz", "rzp", "gain"):
        ids.at(name)
    for p in RELAYED:
        for h in range(2):
            ids.at("zf", p, h)
            for r in range(4):
                ids.at("zs", r, h, p)
    for k in range(9):
        ids.at("w", k)
    return ids


IDS = build_ids()
RINGS = ("ab", "ac", "rb", "rc")
GROUPS = [k + str(h) for k in RINGS for h in range(2)] + ["z", "zp", "zr", "br", "gain", "rz", "rzp", "w", "zf", "zs0", "zs1"]


def kernel(
    hidden_in, gain_in, eid_in, rw_in, len_ref, gate_ref, up_ref, down_ref, sgate_ref, sup_ref, sdown_ref,
    out_ref,
    hbuf, pbuf, rbuf, rown, gbuf, hn, inner, shared, wgu, wd, wsgu, wsd, fc0, fc1, fb, zb, zsum, hidden_ref, eid_ref, rw_ref, isem, lsem, wsem, ssem, rsem,
):
    ep, tp = lax.axis_index("ep"), lax.axis_index("tp")
    z, x = ep // NX, ep % NX
    y, core = tp // 2, tp % 2
    other = 1 - core

    def dev(dz=0, dx=0, dy=0, c=None):
        c = core if c is None else c
        return (((z + dz) % NZ) * NX + (x + dx) % NX, ((y + dy) % NY) * 2 + c)

    barrier = pltpu.get_barrier_semaphore()
    peers = [dev(dz=o, c=c) for o in range(1, NZ) for c in range(2)] + [dev(c=other)]
    peers += [dev(dy=o, c=c) for o in range(1, NY) for c in range(2)]
    peers += [dev(dx=o) for o in range(1, NX)]
    for peer in peers:
        pl.semaphore_signal(barrier, inc=1, device_id=peer, device_id_type=MESH)

    inputs = [
        pltpu.make_async_copy(eid_in, eid_ref, isem.at[0]),
        pltpu.make_async_copy(rw_in, rw_ref, isem.at[1]),
        pltpu.make_async_copy(hidden_in, hidden_ref, isem.at[2]),
        pltpu.make_async_copy(hidden_in.at[core], hbuf.at[core, 0, 0:BLK, 0:HALF], isem.at[3]),
        pltpu.make_async_copy(gain_in, gbuf.at[tp], isem.at[4]),
    ]
    for cp in inputs:
        cp.start()

    def group(key):
        return GROUPS.index(key[0] + str(key[2]) if key[0] in RINGS + ("zs",) else key[0])

    def push(src, dst, key, to, add=0):
        i = IDS.at(*key) + add
        sem = ssem.at[group(key)]
        if key[0] == "w":
            sem = wsem.at[key[1]]
        pltpu.make_async_remote_copy(
            src_ref=src, dst_ref=dst, send_sem=sem, recv_sem=rsem.at[i], device_id=to, device_id_type=MESH
        ).start()

    def sent(ref, sem):
        pltpu.make_async_remote_copy(
            src_ref=ref, dst_ref=ref, send_sem=sem, recv_sem=rsem.at[0], device_id=dev(c=other), device_id_type=MESH
        ).wait_send()

    def arrive(dst, key, add=0):
        i = IDS.at(*key) + add
        pltpu.make_async_remote_copy(
            src_ref=dst, dst_ref=dst, send_sem=ssem.at[0], recv_sem=rsem.at[i], device_id=dev(c=other), device_id_type=MESH
        ).wait_recv()

    def lanes(first):
        return pl.ds(pl.multiple_of(first + core * 128, 128), 128)

    weights = []
    for e in range(2):
        weights.append((gate_ref.at[e], wgu.at[:, lanes(e * 256)]))
        weights.append((up_ref.at[e], wgu.at[:, lanes(512 + e * 256)]))
    weights.append((sgate_ref, wsgu.at[:, lanes(0)]))
    weights.append((sup_ref, wsgu.at[:, lanes(256)]))
    for e in range(2):
        weights.append((down_ref.at[e], wd.at[lanes(e * 256), :]))
    weights.append((sdown_ref, wsd.at[lanes(0), :]))
    local = [pltpu.make_async_copy(s, d, lsem.at[k]) for k, (s, d) in enumerate(weights)]
    for cp in local:
        cp.start()

    def live_slots(shape, dim):
        slot = lax.broadcasted_iota(jnp.int32, shape, dim)
        seq_len = jnp.zeros(shape, jnp.int32)
        for q in range(4):
            seq_len = jnp.where(slot // 8 == q, len_ref[q], seq_len)
        return slot % 8 < seq_len

    for cp in inputs:
        cp.wait()
    expert = lax.broadcasted_iota(jnp.int32, (128, 32), 0)
    mix = jnp.zeros((128, 32), F32)
    for k in range(8):
        mix = mix + jnp.where(eid_ref[k : k + 1, :] == expert % 64, rw_ref[k : k + 1, :], 0.0)
    mix = jnp.where(live_slots((128, 32), 1), mix, 0.0)
    high = mix.astype(BF16).astype(F32)
    terms = jnp.where(expert < 64, high, mix - high).T
    rown[...] = terms.reshape(2, BLK, 128).astype(BF16)
    rbuf[0, 0:BLK, :] = rown[core]

    with jax.named_scope("barrier"):
        pl.semaphore_wait(barrier, len(peers))

    for o in (1, 7, 2, 6, 3, 5, 4):
        p = POS[(-o) % NZ]
        if o == 1:
            push(hidden_ref.at[other], hbuf.at[core, 0, 0:BLK, 0:HALF], ("zp",), dev(c=other), core)
        if p not in RELAYED:
            for c in range(2):
                push(hidden_ref.at[c], hbuf.at[core, p, 0:BLK, 0:HALF], ("z", p, 0), dev(dz=o, c=c), core)
        push(rown.at[core], rbuf.at[p, 0:BLK, :], ("zr", p), dev(dz=o))
    for k, (s, d) in enumerate(weights):
        if k < 4:
            push(s, d, ("w", k), dev(c=other))
    for o in range(NY):
        for c in range(2):
            if o > 0:
                push(gbuf.at[tp], gbuf.at[tp], ("gain",), dev(dy=o, c=c))
    push(gbuf.at[tp], gbuf.at[tp], ("gain",), dev(c=other))
    for k, (s, d) in enumerate(weights):
        if k >= 4:
            push(s, d, ("w", k), dev(c=other))

    def bslice(ref, p, h, r):
        if h == 0:
            return ref.at[h, p, 0:BLK, r * HALF : (r + 1) * HALF]
        return ref.at[h, p, r * BLK : (r + 1) * BLK, 0:HALF]

    def cslice(ref, p, h, r):
        if h == 0:
            return ref.at[h, p, r * BLK : (r + 1) * BLK, :]
        return ref.at[h, p, :, r * HALF : (r + 1) * HALF]

    def pair(view, ref, p, h):
        if view is bslice:
            return ref.at[h, p, 0 : 2 * BLK, 0:HALF] if h == 1 else ref.at[h, p, 0:BLK, 0 : 2 * HALF]
        return ref.at[h, p, 0 : 2 * BLK, :] if h == 0 else ref.at[h, p, :, 0 : 2 * HALF]

    def along(stage, h, step):
        on_y = (stage == "b") == (h == 0)
        return dev(dy=step % NY) if on_y else dev(dx=step % NX)

    def ring_first(view, stage, key, p, h, ref):
        push(view(ref, p, h, 0), view(ref, p, h, 3), (key, p, h, 3), along(stage, h, 1))
        push(view(ref, p, h, 0), view(ref, p, h, 1), (key, p, h, 1), along(stage, h, -1))
        if stage == "b" and p in DIRECT_OUT:
            push(view(ref, p, h, 0), view(ref, p, h, 2), (key, p, h, 2), along(stage, h, 2))

    def ring_forward(view, stage, key, p, h, ref):
        near, step = (3, 1) if p % 2 == 0 else (1, -1)
        arrive(view(ref, p, h, near), (key, p, h, near))
        if stage == "c" or p not in DIRECT_OUT:
            push(view(ref, p, h, near), view(ref, p, h, 2), (key, p, h, 2), along(stage, h, step))

    def ring_done(view, key, p, h, ref):
        arrive(pair(view, ref, p, h), (key, p, h, 2))

    def rslice(p, r):
        return rbuf.at[p, r * BLK : (r + 1) * BLK, :]

    def route_a(p):
        if p > 0:
            arrive(rslice(p, 0), ("zr", p))
        push(rslice(p, 0), rslice(p, 3), ("br", p, 3), dev(dx=1))
        push(rslice(p, 0), rslice(p, 1), ("br", p, 1), dev(dx=3))

    def route_b(p):
        near, step = (3, 1) if p % 2 == 0 else (1, 3)
        arrive(rslice(p, near), ("br", p, near))
        push(rslice(p, near), rslice(p, 2), ("br", p, 2), dev(dx=step))

    def route_c(p):
        arrive(rbuf.at[p, 0 : 2 * BLK, :], ("br", p, 2))

    def gather_a(p, h):
        if p > 0:
            arrive(hbuf.at[h, p, 0:BLK, 0:HALF], ("z", p, h))
        elif h == FIRST_HALF:
            arrive(hbuf.at[other, 0, 0:BLK, 0:HALF], ("zp",), other)
        ring_first(bslice, "b", "ab", p, h, hbuf)

    def gather_b(p, h):
        ring_forward(bslice, "b", "ab", p, h, hbuf)

    def relay(h, slots):
        for p in RELAYED:
            for r in slots:
                push(cslice(hbuf, 0, h, r), cslice(hbuf, p, h, r), ("zf", p, h), dev(dz=-SEQ[p] % NZ))

    def gather_c(p, h):
        ring_done(bslice, "ab", p, h, hbuf)
        ring_first(cslice, "c", "ac", p, h, hbuf)
        if p == 0:
            relay(h, (0,))

    def gather_d(p, h):
        ring_forward(cslice, "c", "ac", p, h, hbuf)
        if p == 0:
            relay(h, (3,))

    def gather_e(p, h):
        if p in RELAYED:
            arrive(hbuf.at[h, p], ("zf", p, h))
            return
        ring_done(cslice, "ac", p, h, hbuf)
        if p == 0:
            relay(h, (1, 2))

    def weight_ready(ks):
        for k in ks:
            local[k].wait()
            arrive(partner[k], ("w", k))

    def plan_partner():
        def lo(first):
            return pl.ds(pl.multiple_of(first + other * 128, 128), 128)

        out = []
        for e in range(2):
            out += [wgu.at[:, lo(e * 256)], wgu.at[:, lo(512 + e * 256)]]
        out += [wsgu.at[:, lo(0)], wsgu.at[:, lo(256)]]
        out += [wd.at[lo(e * 256), :] for e in range(2)]
        return out + [wsd.at[lo(0), :]]

    partner = plan_partner()

    def dot(a, b):
        return jnp.dot(a, b, preferred_element_type=F32)

    def columns(h, r):
        return pl.ds(pl.multiple_of(((y + r) % NY) * 1024 + h * HALF, HALF), HALF)

    def silu(v):
        return v / (1.0 + jnp.exp(-v))

    def normalise(g):
        low, high = GROUPS_OF[g]
        if g == 0:
            arrive(gbuf.at[0:7], ("gain",))

        def block(b, carry):
            p = low + (b // 4) * (high - low)
            at = pl.ds(pl.multiple_of((b % 4) * BLK, BLK), BLK)
            to = pl.ds(pl.multiple_of(b * BLK, BLK), BLK)
            squares = jnp.zeros((BLK, HALF), F32)
            for h in range(2):
                for r in range(NY):
                    v = hbuf[h, p, at, r * HALF : (r + 1) * HALF].astype(F32)
                    squares = squares + v * v
            scale = lax.rsqrt(jnp.sum(squares, axis=1, keepdims=True) / 4096.0 + EPS)
            for h in range(2):
                for r in range(NY):
                    v = hbuf[h, p, at, r * HALF : (r + 1) * HALF].astype(F32)
                    gain = gbuf[((y + r) % NY) * 2 + h]
                    hn[to, columns(h, r)] = (v * scale * gain).astype(BF16)
            return carry

        lax.fori_loop(0, 8, block, 0)

    def hidden_units(g):
        if g == 0:
            weight_ready(range(0, 4))
        route = jnp.concatenate([rbuf[p] for p in GROUPS_OF[g]], axis=0)
        pick_row = lax.broadcasted_iota(jnp.int32, (128, 256), 0) % 64
        for e in range(2):
            pick = jnp.where(pick_row == ep * 2 + e, 1.0, 0.0).astype(BF16)
            share = dot(route, pick)
            gate = dot(hn[...], wgu[:, e * 256 : (e + 1) * 256])
            up = dot(hn[...], wgu[:, 512 + e * 256 : 768 + e * 256])
            inner[:, e * 256 : (e + 1) * 256] = (silu(gate) * up * share).astype(BF16)
        if g == 0:
            weight_ready(range(4, 9))
            own = hn[0:BLK, :]
            shared[...] = (silu(dot(own, wsgu[:, 0:256])) * dot(own, wsgu[:, 256:512])).astype(BF16)

    def outputs(g, h):
        for r in range(NY):
            part = dot(inner[...], wd[:, columns(h, r)])
            cols = slice(r * HALF, (r + 1) * HALF)
            for n, p in enumerate(GROUPS_OF[g]):
                pbuf[h, p, :, cols] = part[n * 64 : (n + 1) * 64].astype(BF16)
                if p == 0:
                    extra = dot(shared[...], wsd[:, columns(h, r)])
                    pbuf[h, 0, 0:BLK, cols] = (part[0:BLK] + extra).astype(BF16)
        for p in GROUPS_OF[g]:
            if p in RELAYED:
                for r in (2, 3, 1, 0):
                    push(cslice(pbuf, p, h, r), cslice(zsum, p - 1, h, r), ("zs", r, h, p), dev(dz=SEQ[p]))

    def relayed(h, r):
        for p in RELAYED:
            arrive(cslice(zsum, p - 1, h, r), ("zs", r, h, p))
        mine = cslice(pbuf, 0, h, r)
        total = mine[...].astype(F32)
        for p in RELAYED:
            total = total + cslice(zsum, p - 1, h, r)[...].astype(F32)
        mine[...] = total.astype(BF16)

    def land(stage, p, h, r):
        if stage == "b":
            return fb.at[h, p, r - 1]
        return (fc0 if h == 0 else fc1).at[p, r - 1]

    def sum_first(view, stage, key, p, h):
        near, step = (1, 1) if p % 2 == 0 else (3, -1)
        if stage == "b" and p in DIRECT_BACK:
            for r in (2, 1, 3):
                push(view(pbuf, p, h, r), land(stage, p, h, 4 - r), (key, p, h, 1), along(stage, h, r))
            return
        push(view(pbuf, p, h, 2), land(stage, p, h, 2), (key, p, h, 2), along(stage, h, step))
        push(view(pbuf, p, h, 4 - near), land(stage, p, h, near), (key, p, h, near), along(stage, h, -step))

    def sum_forward(view, stage, key, p, h):
        near, step = (1, 1) if p % 2 == 0 else (3, -1)
        if stage == "b" and p in DIRECT_BACK:
            return
        arrive(land(stage, p, h, 2), (key, p, h, 2))
        mine = view(pbuf, p, h, near)
        mine[...] = (mine[...].astype(F32) + land(stage, p, h, 2)[...].astype(F32)).astype(BF16)
        push(mine, land(stage, p, h, 4 - near), (key, p, h, 4 - near), along(stage, h, step))

    def sum_last(view, stage, key, p, h):
        whole = fb.at[h, p] if stage == "b" else (fc0 if h == 0 else fc1).at[p]
        direct = stage == "b" and p in DIRECT_BACK
        arrive(whole if direct else whole.at[0:2], (key, p, h, 1))
        mine = view(pbuf, p, h, 0)
        total = mine[...].astype(F32)
        for r in (1, 2, 3) if direct else (1, 3):
            total = total + land(stage, p, h, r)[...].astype(F32)
        mine[...] = total.astype(BF16)

    def sum_r(p, h):
        sum_first(cslice, "c", "rc", p, h)

    def sum_s(p, h):
        sum_forward(cslice, "c", "rc", p, h)

    def sum_t(p, h):
        sum_last(cslice, "c", "rc", p, h)
        sum_first(bslice, "b", "rb", p, h)

    def sum_u(p, h):
        sum_forward(bslice, "b", "rb", p, h)

    def sum_w(p, h):
        sum_last(bslice, "b", "rb", p, h)
        dz = SEQ[p]
        q = POS[(-dz) % NZ]
        if p > 0:
            push(pbuf.at[h, p, 0:BLK, 0:HALF], zb.at[q, core], ("rz",), dev(dz=dz, c=h))
        elif h == LAST_HALF:
            zb[0, core] = pbuf[core, 0, 0:BLK, 0:HALF]
            push(pbuf.at[other, 0, 0:BLK, 0:HALF], zb.at[0, core], ("rzp",), dev(c=other))

    steps = dict(i=route_a, j=route_b, k=route_c, a=gather_a, b=gather_b, c=gather_c, d=gather_d, e=gather_e)
    steps |= dict(n=normalise, m=hidden_units, v=outputs, q=relayed, r=sum_r, s=sum_s, t=sum_t, u=sum_u, w=sum_w)
    for name in ORDER:
        with jax.named_scope(name):
            steps[name[0]](*[int(digit) for digit in name[1:]])

    with jax.named_scope("final"):
        arrive(zb.at[1 : len(PLANES)], ("rz",))
        arrive(zb.at[0, other], ("rzp",))
    live = live_slots((2 * BLK, HALF), 0)
    for c in range(2):
        total = zb[0, c].astype(F32)
        for p in PLANES[1:]:
            total = total + zb[p, c].astype(F32)
        alive = live[c * BLK : (c + 1) * BLK]
        out_ref[c] = jnp.where(alive, total, 0.0).astype(BF16)
    with jax.named_scope("drain"):
        n = len(PLANES)
        rings = {"zp": zb.at[0, 0], "rzp": zb.at[0, 0], "z": zb.at[1:n], "rz": zb.at[1:n]}
        rings |= {"zr": rbuf.at[0:7, 0:BLK, :], "br": rbuf.at[:, 0:48, :], "gain": gbuf.at[0:7]}
        for h in range(2):
            rings |= {f"ab{h}": fb.at[h, 0:n], f"rb{h}": fb.at[h, 0:n]}
            rings |= {f"ac{h}": (fc0, fc1)[h].at[0:n], f"rc{h}": (fc0, fc1)[h].at[0:n]}
            if RELAYED:
                rings[f"zs{h}"] = hbuf.at[h, 0 : len(RELAYED)]
        if RELAYED:
            rings["zf"] = hbuf.at[:, 0 : len(RELAYED)]
        for name, ref in rings.items():
            sent(ref, ssem.at[GROUPS.index(name)])
        for k, (s, _) in enumerate(weights):
            sent(s, wsem.at[k])


def body(hidden, norm_gain, expert_ids, route_weights, lengths, gate_proj, up_proj, down_proj, sgate, sup, sdown):
    vmem = pl.BlockSpec(memory_space=pltpu.VMEM)
    anywhere = pl.BlockSpec(memory_space=pl.ANY)
    n = IDS.count
    out = pl.pallas_call(
        kernel,
        out_shape=jax.ShapeDtypeStruct((2, BLK, HALF), BF16),
        in_specs=[anywhere] * 4 + [pl.BlockSpec(memory_space=pltpu.SMEM)] + [anywhere] * 6,
        out_specs=vmem,
        scratch_shapes=[
            pltpu.VMEM((2, NZ, 64, 2048), BF16),
            pltpu.VMEM((2, NZ, 64, 2048), BF16),
            pltpu.VMEM((NZ, 64, 128), BF16),
            pltpu.VMEM((2, BLK, 128), BF16),
            pltpu.VMEM((8, 1, HALF), F32),
            pltpu.VMEM((128, 4096), BF16),
            pltpu.VMEM((128, 512), BF16),
            pltpu.VMEM((BLK, 256), BF16),
            pltpu.VMEM((4096, 1024), BF16),
            pltpu.VMEM((512, 4096), BF16),
            pltpu.VMEM((4096, 512), BF16),
            pltpu.VMEM((256, 4096), BF16),
            pltpu.VMEM((NZ, 3, BLK, 2048), BF16),
            pltpu.VMEM((NZ, 3, 64, HALF), BF16),
            pltpu.VMEM((2, NZ, 3, BLK, HALF), BF16),
            pltpu.VMEM((NZ, 2, BLK, HALF), BF16),
            pltpu.VMEM((2, 2, 64, 2048), BF16),
            pltpu.VMEM((2, BLK, HALF), BF16),
            pltpu.VMEM((8, 32), jnp.int32),
            pltpu.VMEM((8, 32), F32),
            pltpu.SemaphoreType.DMA((5,)),
            pltpu.SemaphoreType.DMA((9,)),
            pltpu.SemaphoreType.DMA((9,)),
            pltpu.SemaphoreType.DMA((len(GROUPS),)),
            pltpu.SemaphoreType.DMA((n,)),
        ],
        compiler_params=pltpu.CompilerParams(
            collective_id=0, has_side_effects=True, vmem_limit_bytes=60 * 1024 * 1024
        ),
    )(
        hidden.reshape(2, BLK, HALF),
        norm_gain.reshape(1, HALF),
        expert_ids.T,
        route_weights.T,
        lengths,
        gate_proj,
        up_proj,
        down_proj,
        sgate,
        sup,
        sdown,
    )
    return out.reshape(2 * BLK, HALF)


def solution(mesh):
    placed = (
        P("ep", "tp"),
        P("tp"),
        P("ep", None),
        P("ep", None),
        P("ep"),
        P("ep", None, "tp"),
        P("ep", None, "tp"),
        P("ep", "tp", None),
        P(None, "tp"),
        P(None, "tp"),
        P("tp", None),
    )
    return jax.shard_map(body, mesh=mesh, in_specs=placed, out_specs=P("ep", "tp"), check_vma=False)
```

```python
import functools

import jax
import jax.numpy as jnp
from jax import lax
from jax.experimental import pallas as pl
from jax.experimental.pallas import tpu as pltpu
from jax.sharding import PartitionSpec as P

MESH = pl.DeviceIdType.MESH
EPS = 1e-06
NZ, NX, NY = 8, 4, 4
BLK = 16
HALF = 512
F32, BF16 = jnp.float32, jnp.bfloat16
SEQ = (0, 1, 7, 2, 6, 3, 5, 4)
POS = {dz: i for i, dz in enumerate(SEQ)}


GROUPS_OF = ((0, 3), (4, 5), (1, 2), (6, 7))
ORDER = (
    "a00", "a01", "y", "b01", "b00", "c00", "c01", "a31", "a30", "a50", "i5", "i2", "i4", "i3", "a41", "a40",
    "a61", "a60", "a51", "i0", "i6", "i1", "d01", "a71", "a70", "b30", "d00", "i7", "b41", "b31", "c31", "c30",
    "b51", "c41", "b50", "j6", "b71", "b70", "b40", "j3", "j4", "j7", "c40", "j5", "j2", "b60", "e01", "b61",
    "e00", "n0", "j1", "d31", "d30", "j0", "c50", "c51", "c60", "k3", "k5", "d40", "c61", "x", "c70", "e11",
    "k1", "k4", "e21", "d41", "k0", "c71", "k7", "k2", "k6", "e31", "e30", "n3", "m01", "m00", "d50", "d51",
    "v00", "e10", "v01", "e20", "n1", "r31", "r30", "d60", "n2", "d61", "m21", "d70", "d71", "m20", "e40", "v21",
    "v20", "e41", "e51", "e50", "n4", "n5", "m10", "s31", "m11", "v11", "r41", "v10", "r50", "r51", "e71", "e60",
    "e61", "e70", "n7", "n6", "r40", "m30", "m31", "v31", "r71", "t31", "v30", "r70", "r61", "q11", "s41", "s50",
    "s30", "r60", "s51", "q13", "s40", "q12", "s71", "r01", "q02", "q03", "s70", "r00", "s61", "u31", "s60", "t50",
    "t41", "t51", "q01", "t30", "t40", "t71", "s01", "s00", "t70", "q10", "t60", "t61", "u40", "u41", "u51", "u50",
    "w50", "u30", "t01", "q00", "w51", "u71", "t00", "u70", "w71", "w70", "u60", "w60", "u61", "w61", "w40", "w31",
    "w30", "w41", "u01", "w01", "u00", "w00",
)
RELAYED = (1, 2)
DIRECT_OUT = (0, 3, 4)
DIRECT_BACK = (0, 5, 6, 7)
PLANES = tuple(p for p in range(8) if p not in RELAYED)
FIRST_HALF = 0 if ORDER.index("a00") < ORDER.index("a01") else 1
LAST_HALF = 1 if ORDER.index("w00") < ORDER.index("w01") else 0


def shared_key(key):
    if key[0] in ("ab", "ac"):
        return key if key[3] == (3 if key[1] % 2 == 0 else 1) else key[:3] + (2,)
    if key[0] in ("rb", "rc"):
        direct = key[0] == "rb" and key[1] in DIRECT_BACK
        return key[:3] + (1,) if direct or key[3] != 2 else key
    if key[0] == "br":
        return key if key[2] == (3 if key[1] % 2 == 0 else 1) else key[:2] + (2,)
    if key[0] == "rz":
        return ("rz",)
    return key


class Ids:
    def __init__(self):
        self.table, self.count = {}, 0

    def at(self, *key):
        key = shared_key(key)
        if key not in self.table:
            self.table[key] = self.count
            self.count += 1
        return self.table[key]


def build_ids():
    ids = Ids()
    ids.count = ids.at("zp") + 2
    for p in range(NZ):
        for h in range(2):
            ids.at("z", p, h)
    for p in range(NZ):
        ids.at("zr", p)
        for r in (1, 2, 3):
            ids.at("br", p, r)
            for h in range(2):
                for stage in ("ab", "ac", "rc", "rb"):
                    if p not in RELAYED:
                        ids.at(stage, p, h, r)
    for name in ("rz", "rzp", "gain"):
        ids.at(name)
    for p in RELAYED:
        for h in range(2):
            ids.at("zf", p, h)
            for r in range(4):
                ids.at("zs", r, h, p)
    for k in range(9):
        ids.at("w", k)
    return ids


IDS = build_ids()
RINGS = ("ab", "ac", "rb", "rc")
GROUPS = [k + str(h) for k in RINGS for h in range(2)] + ["z", "zp", "zr", "br", "gain", "rz", "rzp", "w", "zf", "zs0", "zs1"]


def kernel(
    hidden_in, gain_in, eid_in, rw_in, len_ref, gate_ref, up_ref, down_ref, sgate_ref, sup_ref, sdown_ref,
    out_ref,
    hbuf, pbuf, rbuf, rown, gbuf, hn, inner, shared, wgu, wd, wsgu, wsd, fc0, fc1, fb, zb, zsum, hidden_ref, eid_ref, rw_ref, isem, lsem, wsem, ssem, rsem,
):
    ep, tp = lax.axis_index("ep"), lax.axis_index("tp")
    z, x = ep // NX, ep % NX
    y, core = tp // 2, tp % 2
    other = 1 - core

    def dev(dz=0, dx=0, dy=0, c=None):
        c = core if c is None else c
        return (((z + dz) % NZ) * NX + (x + dx) % NX, ((y + dy) % NY) * 2 + c)

    inputs = [
        pltpu.make_async_copy(hidden_in, hidden_ref, isem.at[0]),
        pltpu.make_async_copy(hidden_in.at[core], hbuf.at[core, 0, 0:BLK, 0:HALF], isem.at[1]),
        pltpu.make_async_copy(gain_in, gbuf.at[tp], isem.at[2]),
        pltpu.make_async_copy(eid_in, eid_ref, isem.at[3]),
        pltpu.make_async_copy(rw_in, rw_ref, isem.at[4]),
    ]
    for cp in inputs:
        cp.start()

    barrier = pltpu.get_barrier_semaphore()
    peers = [dev(dz=o, c=c) for o in range(1, NZ) for c in range(2)] + [dev(c=other)]
    peers += [dev(dy=o, c=c) for o in range(1, NY) for c in range(2)]
    peers += [dev(dx=o) for o in range(1, NX)]
    for peer in peers:
        pl.semaphore_signal(barrier, inc=1, device_id=peer, device_id_type=MESH)

    def group(key):
        return GROUPS.index(key[0] + str(key[2]) if key[0] in RINGS + ("zs",) else key[0])

    def push(src, dst, key, to, add=0):
        i = IDS.at(*key) + add
        sem = ssem.at[group(key)]
        if key[0] == "w":
            sem = wsem.at[key[1]]
        pltpu.make_async_remote_copy(
            src_ref=src, dst_ref=dst, send_sem=sem, recv_sem=rsem.at[i], device_id=to, device_id_type=MESH
        ).start()

    def sent(ref, sem):
        pltpu.make_async_remote_copy(
            src_ref=ref, dst_ref=ref, send_sem=sem, recv_sem=rsem.at[0], device_id=dev(c=other), device_id_type=MESH
        ).wait_send()

    def arrive(dst, key, add=0):
        i = IDS.at(*key) + add
        pltpu.make_async_remote_copy(
            src_ref=dst, dst_ref=dst, send_sem=ssem.at[0], recv_sem=rsem.at[i], device_id=dev(c=other), device_id_type=MESH
        ).wait_recv()

    def lanes(first):
        return pl.ds(pl.multiple_of(first + core * 128, 128), 128)

    weights = []
    for e in range(2):
        weights.append((gate_ref.at[e], wgu.at[:, lanes(e * 256)]))
        weights.append((up_ref.at[e], wgu.at[:, lanes(512 + e * 256)]))
    weights.append((sgate_ref, wsgu.at[:, lanes(0)]))
    weights.append((sup_ref, wsgu.at[:, lanes(256)]))
    for e in range(2):
        weights.append((down_ref.at[e], wd.at[lanes(e * 256), :]))
    weights.append((sdown_ref, wsd.at[lanes(0), :]))
    local = [pltpu.make_async_copy(s, d, lsem.at[k]) for k, (s, d) in enumerate(weights)]
    def live_slots(shape, dim):
        slot = lax.broadcasted_iota(jnp.int32, shape, dim)
        seq_len = jnp.zeros(shape, jnp.int32)
        for q in range(4):
            seq_len = jnp.where(slot // 8 == q, len_ref[q], seq_len)
        return slot % 8 < seq_len

    with jax.named_scope("inputs"):
        for cp in inputs[:3]:
            cp.wait()
    for cp in local:
        cp.start()

    with jax.named_scope("barrier"):
        pl.semaphore_wait(barrier, len(peers))

    for o in (1, 7, 2, 6, 3, 5, 4):
        p = POS[(-o) % NZ]
        if o == 1:
            push(hidden_ref.at[other], hbuf.at[core, 0, 0:BLK, 0:HALF], ("zp",), dev(c=other), core)
        if p not in RELAYED:
            for c in range(2):
                push(hidden_ref.at[c], hbuf.at[core, p, 0:BLK, 0:HALF], ("z", p, 0), dev(dz=o, c=c), core)
    for k, (s, d) in enumerate(weights):
        if k < 4:
            push(s, d, ("w", k), dev(c=other))
    for o in range(NY):
        for c in range(2):
            if o > 0:
                push(gbuf.at[tp], gbuf.at[tp], ("gain",), dev(dy=o, c=c))
    push(gbuf.at[tp], gbuf.at[tp], ("gain",), dev(c=other))
    for k, (s, d) in enumerate(weights):
        if k >= 4:
            push(s, d, ("w", k), dev(c=other))

    def bslice(ref, p, h, r):
        if h == 0:
            return ref.at[h, p, 0:BLK, r * HALF : (r + 1) * HALF]
        return ref.at[h, p, r * BLK : (r + 1) * BLK, 0:HALF]

    def cslice(ref, p, h, r):
        if h == 0:
            return ref.at[h, p, r * BLK : (r + 1) * BLK, :]
        return ref.at[h, p, :, r * HALF : (r + 1) * HALF]

    def pair(view, ref, p, h):
        if view is bslice:
            return ref.at[h, p, 0 : 2 * BLK, 0:HALF] if h == 1 else ref.at[h, p, 0:BLK, 0 : 2 * HALF]
        return ref.at[h, p, 0 : 2 * BLK, :] if h == 0 else ref.at[h, p, :, 0 : 2 * HALF]

    def along(stage, h, step):
        on_y = (stage == "b") == (h == 0)
        return dev(dy=step % NY) if on_y else dev(dx=step % NX)

    def ring_first(view, stage, key, p, h, ref):
        push(view(ref, p, h, 0), view(ref, p, h, 3), (key, p, h, 3), along(stage, h, 1))
        push(view(ref, p, h, 0), view(ref, p, h, 1), (key, p, h, 1), along(stage, h, -1))
        if stage == "b" and p in DIRECT_OUT:
            push(view(ref, p, h, 0), view(ref, p, h, 2), (key, p, h, 2), along(stage, h, 2))

    def ring_forward(view, stage, key, p, h, ref):
        near, step = (3, 1) if p % 2 == 0 else (1, -1)
        arrive(view(ref, p, h, near), (key, p, h, near))
        if stage == "c" or p not in DIRECT_OUT:
            push(view(ref, p, h, near), view(ref, p, h, 2), (key, p, h, 2), along(stage, h, step))

    def ring_done(view, key, p, h, ref):
        arrive(pair(view, ref, p, h), (key, p, h, 2))

    def rslice(p, r):
        return rbuf.at[p, r * BLK : (r + 1) * BLK, :]

    def route_start():
        for cp in inputs[3:]:
            cp.wait()
        expert = lax.broadcasted_iota(jnp.int32, (128, 32), 0)
        mix = jnp.zeros((128, 32), F32)
        for k in range(8):
            mix = mix + jnp.where(eid_ref[k : k + 1, :] == expert % 64, rw_ref[k : k + 1, :], 0.0)
        mix = jnp.where(live_slots((128, 32), 1), mix, 0.0)
        high = mix.astype(BF16).astype(F32)
        terms = jnp.where(expert < 64, high, mix - high).T
        rown[...] = terms.reshape(2, BLK, 128).astype(BF16)
        rbuf[0, 0:BLK, :] = rown[core]
        for o in range(1, NZ):
            push(rown.at[core], rbuf.at[POS[-o % NZ], 0:BLK, :], ("zr", POS[-o % NZ]), dev(dz=o))

    def route_a(p):
        if p > 0:
            arrive(rslice(p, 0), ("zr", p))
        push(rslice(p, 0), rslice(p, 3), ("br", p, 3), dev(dx=1))
        push(rslice(p, 0), rslice(p, 1), ("br", p, 1), dev(dx=3))

    def route_b(p):
        near, step = (3, 1) if p % 2 == 0 else (1, 3)
        arrive(rslice(p, near), ("br", p, near))
        push(rslice(p, near), rslice(p, 2), ("br", p, 2), dev(dx=step))

    def route_c(p):
        arrive(rbuf.at[p, 0 : 2 * BLK, :], ("br", p, 2))

    def gather_a(p, h):
        if p > 0:
            arrive(hbuf.at[h, p, 0:BLK, 0:HALF], ("z", p, h))
        elif h == FIRST_HALF:
            arrive(hbuf.at[other, 0, 0:BLK, 0:HALF], ("zp",), other)
        ring_first(bslice, "b", "ab", p, h, hbuf)

    def gather_b(p, h):
        ring_forward(bslice, "b", "ab", p, h, hbuf)

    def relay(h, slots):
        for p in RELAYED:
            for r in slots:
                push(cslice(hbuf, 0, h, r), cslice(hbuf, p, h, r), ("zf", p, h), dev(dz=-SEQ[p] % NZ))

    def gather_c(p, h):
        ring_done(bslice, "ab", p, h, hbuf)
        ring_first(cslice, "c", "ac", p, h, hbuf)
        if p == 0:
            relay(h, (0,))

    def gather_d(p, h):
        ring_forward(cslice, "c", "ac", p, h, hbuf)
        if p == 0:
            relay(h, (3,))

    def gather_e(p, h):
        if p in RELAYED:
            arrive(hbuf.at[h, p], ("zf", p, h))
            return
        ring_done(cslice, "ac", p, h, hbuf)
        if p == 0:
            relay(h, (1, 2))

    def weight_ready(ks):
        for k in ks:
            local[k].wait()
            arrive(partner[k], ("w", k))

    def plan_partner():
        def lo(first):
            return pl.ds(pl.multiple_of(first + other * 128, 128), 128)

        out = []
        for e in range(2):
            out += [wgu.at[:, lo(e * 256)], wgu.at[:, lo(512 + e * 256)]]
        out += [wsgu.at[:, lo(0)], wsgu.at[:, lo(256)]]
        out += [wd.at[lo(e * 256), :] for e in range(2)]
        return out + [wsd.at[lo(0), :]]

    partner = plan_partner()

    def dot(a, b):
        return jnp.dot(a, b, preferred_element_type=F32)

    def columns(h, r):
        return pl.ds(pl.multiple_of(((y + r) % NY) * 1024 + h * HALF, HALF), HALF)

    def silu(v):
        return v / (1.0 + jnp.exp(-v))

    firsts = {letter: next(n for n in ORDER if n[0] == letter) for letter in "nmv"}

    def normalise(p):
        g = next(k for k, planes in enumerate(GROUPS_OF) if p in planes)
        offset = GROUPS_OF[g].index(p) * 64
        if firsts["n"] == f"n{p}":
            arrive(gbuf.at[0:7], ("gain",))

        def block(b, carry):
            at = pl.ds(pl.multiple_of(b * BLK, BLK), BLK)
            to = pl.ds(pl.multiple_of(offset + b * BLK, BLK), BLK)
            squares = jnp.zeros((BLK, HALF), F32)
            for h in range(2):
                for r in range(NY):
                    v = hbuf[h, p, at, r * HALF : (r + 1) * HALF].astype(F32)
                    squares = squares + v * v
            scale = lax.rsqrt(jnp.sum(squares, axis=1, keepdims=True) / 4096.0 + EPS)
            for h in range(2):
                for r in range(NY):
                    v = hbuf[h, p, at, r * HALF : (r + 1) * HALF].astype(F32)
                    gain = gbuf[((y + r) % NY) * 2 + h]
                    hn[g, to, columns(h, r)] = (v * scale * gain).astype(BF16)
            return carry

        lax.fori_loop(0, 4, block, 0)

    def hidden_units(g, e):
        if firsts["m"] == f"m{g}{e}":
            weight_ready(range(0, 4))
        route = jnp.concatenate([rbuf[p] for p in GROUPS_OF[g]], axis=0)
        pick_row = lax.broadcasted_iota(jnp.int32, (128, 256), 0) % 64
        pick = jnp.where(pick_row == ep * 2 + e, 1.0, 0.0).astype(BF16)
        share = dot(route, pick)
        gate = dot(hn[g], wgu[:, e * 256 : (e + 1) * 256])
        up = dot(hn[g], wgu[:, 512 + e * 256 : 768 + e * 256])
        inner[g, :, e * 256 : (e + 1) * 256] = (silu(gate) * up * share).astype(BF16)

    def shared_units():
        weight_ready(range(4, 6))
        g = next(k for k, planes in enumerate(GROUPS_OF) if 0 in planes)
        own = hn[g, 0:BLK, :]
        shared[...] = (silu(dot(own, wsgu[:, 0:256])) * dot(own, wsgu[:, 256:512])).astype(BF16)

    def outputs(g, h):
        if firsts["v"] == f"v{g}{h}":
            weight_ready(range(6, 9))
        for r in range(NY):
            part = dot(inner[g], wd[:, columns(h, r)])
            cols = slice(r * HALF, (r + 1) * HALF)
            for n, p in enumerate(GROUPS_OF[g]):
                pbuf[h, p, :, cols] = part[n * 64 : (n + 1) * 64].astype(BF16)
                if p == 0:
                    extra = dot(shared[...], wsd[:, columns(h, r)])
                    pbuf[h, 0, 0:BLK, cols] = (part[0:BLK] + extra).astype(BF16)
        for p in GROUPS_OF[g]:
            if p in RELAYED:
                for r in (2, 3, 1, 0):
                    push(cslice(pbuf, p, h, r), cslice(zsum, p - 1, h, r), ("zs", r, h, p), dev(dz=SEQ[p]))

    def relayed(h, r):
        for p in RELAYED:
            arrive(cslice(zsum, p - 1, h, r), ("zs", r, h, p))
        mine = cslice(pbuf, 0, h, r)
        total = mine[...].astype(F32)
        for p in RELAYED:
            total = total + cslice(zsum, p - 1, h, r)[...].astype(F32)
        mine[...] = total.astype(BF16)

    def land(stage, p, h, r):
        if stage == "b":
            return fb.at[h, p, r - 1]
        return (fc0 if h == 0 else fc1).at[p, r - 1]

    def sum_first(view, stage, key, p, h):
        near, step = (1, 1) if p % 2 == 0 else (3, -1)
        if stage == "b" and p in DIRECT_BACK:
            for r in (2, 1, 3):
                push(view(pbuf, p, h, r), land(stage, p, h, 4 - r), (key, p, h, 1), along(stage, h, r))
            return
        push(view(pbuf, p, h, 2), land(stage, p, h, 2), (key, p, h, 2), along(stage, h, step))
        push(view(pbuf, p, h, 4 - near), land(stage, p, h, near), (key, p, h, near), along(stage, h, -step))

    def sum_forward(view, stage, key, p, h):
        near, step = (1, 1) if p % 2 == 0 else (3, -1)
        if stage == "b" and p in DIRECT_BACK:
            return
        arrive(land(stage, p, h, 2), (key, p, h, 2))
        mine = view(pbuf, p, h, near)
        mine[...] = (mine[...].astype(F32) + land(stage, p, h, 2)[...].astype(F32)).astype(BF16)
        push(mine, land(stage, p, h, 4 - near), (key, p, h, 4 - near), along(stage, h, step))

    def sum_last(view, stage, key, p, h):
        whole = fb.at[h, p] if stage == "b" else (fc0 if h == 0 else fc1).at[p]
        direct = stage == "b" and p in DIRECT_BACK
        arrive(whole if direct else whole.at[0:2], (key, p, h, 1))
        mine = view(pbuf, p, h, 0)
        total = mine[...].astype(F32)
        for r in (1, 2, 3) if direct else (1, 3):
            total = total + land(stage, p, h, r)[...].astype(F32)
        mine[...] = total.astype(BF16)

    def sum_r(p, h):
        sum_first(cslice, "c", "rc", p, h)

    def sum_s(p, h):
        sum_forward(cslice, "c", "rc", p, h)

    def sum_t(p, h):
        sum_last(cslice, "c", "rc", p, h)
        sum_first(bslice, "b", "rb", p, h)

    def sum_u(p, h):
        sum_forward(bslice, "b", "rb", p, h)

    def sum_w(p, h):
        sum_last(bslice, "b", "rb", p, h)
        dz = SEQ[p]
        q = POS[(-dz) % NZ]
        if p > 0:
            push(pbuf.at[h, p, 0:BLK, 0:HALF], zb.at[q, core], ("rz",), dev(dz=dz, c=h))
        elif h == LAST_HALF:
            zb[0, core] = pbuf[core, 0, 0:BLK, 0:HALF]
            push(pbuf.at[other, 0, 0:BLK, 0:HALF], zb.at[0, core], ("rzp",), dev(c=other))

    steps = dict(y=route_start, i=route_a, j=route_b, k=route_c, a=gather_a, b=gather_b, c=gather_c, d=gather_d, e=gather_e)
    steps |= dict(n=normalise, m=hidden_units, x=shared_units, v=outputs, q=relayed, r=sum_r, s=sum_s, t=sum_t, u=sum_u, w=sum_w)
    for name in ORDER:
        with jax.named_scope(name):
            steps[name[0]](*[int(digit) for digit in name[1:]])

    with jax.named_scope("final"):
        arrive(zb.at[1 : len(PLANES)], ("rz",))
        arrive(zb.at[0, other], ("rzp",))
    live = live_slots((2 * BLK, HALF), 0)
    for c in range(2):
        total = zb[0, c].astype(F32)
        for p in PLANES[1:]:
            total = total + zb[p, c].astype(F32)
        alive = live[c * BLK : (c + 1) * BLK]
        out_ref[c] = jnp.where(alive, total, 0.0).astype(BF16)
    with jax.named_scope("drain"):
        n = len(PLANES)
        rings = {"zp": zb.at[0, 0], "rzp": zb.at[0, 0], "z": zb.at[1:n], "rz": zb.at[1:n]}
        rings |= {"zr": rbuf.at[0:7, 0:BLK, :], "br": rbuf.at[:, 0:48, :], "gain": gbuf.at[0:7]}
        for h in range(2):
            rings |= {f"ab{h}": fb.at[h, 0:n], f"rb{h}": fb.at[h, 0:n]}
            rings |= {f"ac{h}": (fc0, fc1)[h].at[0:n], f"rc{h}": (fc0, fc1)[h].at[0:n]}
            if RELAYED:
                rings[f"zs{h}"] = hbuf.at[h, 0 : len(RELAYED)]
        if RELAYED:
            rings["zf"] = hbuf.at[:, 0 : len(RELAYED)]
        for name, ref in rings.items():
            sent(ref, ssem.at[GROUPS.index(name)])
        for k, (s, _) in enumerate(weights):
            sent(s, wsem.at[k])


def body(hidden, norm_gain, expert_ids, route_weights, lengths, gate_proj, up_proj, down_proj, sgate, sup, sdown):
    vmem = pl.BlockSpec(memory_space=pltpu.VMEM)
    anywhere = pl.BlockSpec(memory_space=pltpu.HBM)
    n = IDS.count
    out = pl.pallas_call(
        kernel,
        out_shape=jax.ShapeDtypeStruct((2, BLK, HALF), BF16),
        in_specs=[anywhere] * 4 + [pl.BlockSpec(memory_space=pltpu.SMEM)] + [anywhere] * 6,
        out_specs=vmem,
        scratch_shapes=[
            pltpu.VMEM((2, NZ, 64, 2048), BF16),
            pltpu.VMEM((2, NZ, 64, 2048), BF16),
            pltpu.VMEM((NZ, 64, 128), BF16),
            pltpu.VMEM((2, BLK, 128), BF16),
            pltpu.VMEM((8, 1, HALF), F32),
            pltpu.VMEM((4, 128, 4096), BF16),
            pltpu.VMEM((4, 128, 512), BF16),
            pltpu.VMEM((BLK, 256), BF16),
            pltpu.VMEM((4096, 1024), BF16),
            pltpu.VMEM((512, 4096), BF16),
            pltpu.VMEM((4096, 512), BF16),
            pltpu.VMEM((256, 4096), BF16),
            pltpu.VMEM((NZ, 3, BLK, 2048), BF16),
            pltpu.VMEM((NZ, 3, 64, HALF), BF16),
            pltpu.VMEM((2, NZ, 3, BLK, HALF), BF16),
            pltpu.VMEM((NZ, 2, BLK, HALF), BF16),
            pltpu.VMEM((2, 2, 64, 2048), BF16),
            pltpu.VMEM((2, BLK, HALF), BF16),
            pltpu.VMEM((8, 32), jnp.int32),
            pltpu.VMEM((8, 32), F32),
            pltpu.SemaphoreType.DMA((5,)),
            pltpu.SemaphoreType.DMA((9,)),
            pltpu.SemaphoreType.DMA((9,)),
            pltpu.SemaphoreType.DMA((len(GROUPS),)),
            pltpu.SemaphoreType.DMA((n,)),
        ],
        compiler_params=pltpu.CompilerParams(
            collective_id=0, has_side_effects=True, vmem_limit_bytes=60 * 1024 * 1024
        ),
    )(
        hidden.reshape(2, BLK, HALF),
        norm_gain.reshape(1, HALF),
        expert_ids.T,
        route_weights.T,
        lengths,
        gate_proj,
        up_proj,
        down_proj,
        sgate,
        sup,
        sdown,
    )
    return out.reshape(2 * BLK, HALF)


def solution(mesh):
    placed = (
        P("ep", "tp"),
        P("tp"),
        P("ep", None),
        P("ep", None),
        P("ep"),
        P("ep", None, "tp"),
        P("ep", None, "tp"),
        P("ep", "tp", None),
        P(None, "tp"),
        P(None, "tp"),
        P("tp", None),
    )
    return jax.shard_map(body, mesh=mesh, in_specs=placed, out_specs=P("ep", "tp"), check_vma=False)
```

```python
import functools

import jax
import jax.numpy as jnp
from jax import lax
from jax.experimental import pallas as pl
from jax.experimental.pallas import tpu as pltpu
from jax.sharding import PartitionSpec as P

MESH = pl.DeviceIdType.MESH
EPS = 1e-06
NZ, NX, NY = 8, 4, 4
BLK = 16
HALF = 512
F32, BF16 = jnp.float32, jnp.bfloat16
SEQ = (0, 1, 7, 2, 6, 3, 5, 4)
POS = {dz: i for i, dz in enumerate(SEQ)}


GROUPS_OF = ((0, 3), (4, 5), (1, 2), (6, 7))
ORDER = (
    "a01", "a00", "y", "b01", "c01", "a31", "a30", "i1", "a51", "a40", "i0", "b00", "i3", "i2", "a60", "c00",
    "a50", "a61", "a71", "d01", "b31", "a70", "j1", "i5", "i4", "b30", "b51", "a41", "i7", "c31", "c30", "b40",
    "d00", "j5", "b71", "b50", "j0", "b61", "c51", "j2", "e01", "i6", "b41", "j7", "c40", "j3", "b60", "b70",
    "d31", "k1", "c41", "d30", "k5", "j4", "e00", "c50", "c61", "n0", "x", "k7", "c71", "c60", "d40", "e11",
    "e21", "j6", "k2", "k3", "c70", "k4", "e31", "k0", "d41", "d51", "e30", "n3", "m01", "m00", "d50", "v01",
    "d61", "v00", "r31", "e10", "e20", "n2", "r30", "n1", "d60", "d71", "m20", "d70", "m21", "v21", "e51", "v20",
    "e41", "k6", "e50", "n5", "e40", "e61", "n4", "m11", "s31", "s30", "m10", "v11", "r51", "v10", "e71", "r41",
    "r50", "r40", "e70", "e60", "n6", "n7", "m30", "m31", "v30", "r70", "t30", "v31", "r71", "s51", "r60", "q13",
    "r61", "s41", "q12", "s50", "s40", "q02", "q03", "s70", "r00", "s71", "r01", "q01", "s60", "s61", "q11", "t51",
    "t31", "q10", "u30", "t50", "t41", "t40", "t70", "s00", "s01", "t71", "u31", "q00", "t60", "u51", "t61", "u50",
    "u41", "u40", "u70", "t00", "t01", "u71", "w70", "w30", "w50", "w31", "w71", "w51", "w40", "u60", "w60", "u61",
    "w61", "w41", "u00", "w00", "u01", "w01",
)
RELAYED = (1, 2)
DIRECT_OUT = (0, 3, 4)
DIRECT_BACK = (0, 6, 7)
PLANES = tuple(p for p in range(8) if p not in RELAYED)
FIRST_HALF = 0 if ORDER.index("a00") < ORDER.index("a01") else 1
LAST_HALF = 1 if ORDER.index("w00") < ORDER.index("w01") else 0


def shared_key(key):
    if key[0] in ("ab", "ac"):
        return key if key[3] == (3 if key[1] % 2 == 0 else 1) else key[:3] + (2,)
    if key[0] in ("rb", "rc"):
        direct = key[0] == "rb" and key[1] in DIRECT_BACK
        return key[:3] + (1,) if direct or key[3] != 2 else key
    if key[0] == "br":
        return key if key[2] == (3 if key[1] % 2 == 0 else 1) else key[:2] + (2,)
    if key[0] == "rz":
        return ("rz",)
    return key


class Ids:
    def __init__(self):
        self.table, self.count = {}, 0

    def at(self, *key):
        key = shared_key(key)
        if key not in self.table:
            self.table[key] = self.count
            self.count += 1
        return self.table[key]


def build_ids():
    ids = Ids()
    ids.count = ids.at("zp") + 2
    for p in range(NZ):
        for h in range(2):
            ids.at("z", p, h)
    for p in range(NZ):
        ids.at("zr", p)
        for r in (1, 2, 3):
            ids.at("br", p, r)
            for h in range(2):
                for stage in ("ab", "ac", "rc", "rb"):
                    if p not in RELAYED:
                        ids.at(stage, p, h, r)
    for name in ("rz", "rzp", "gain"):
        ids.at(name)
    for p in RELAYED:
        for h in range(2):
            ids.at("zf", p, h)
            for r in range(4):
                ids.at("zs", r, h, p)
    for k in range(9):
        ids.at("w", k)
    return ids


IDS = build_ids()
RINGS = ("ab", "ac", "rb", "rc")
GROUPS = [k + str(h) for k in RINGS for h in range(2)] + ["z", "zp", "zr", "br", "gain", "rz", "rzp", "w", "zf", "zs0", "zs1"]


def kernel(
    hidden_in, gain_in, eid_in, rw_in, len_ref, gate_ref, up_ref, down_ref, sgate_ref, sup_ref, sdown_ref,
    out_ref,
    hbuf, pbuf, rbuf, rown, gbuf, hn, inner, shared, wgu, wd, wsgu, wsd, fc0, fc1, fb, zb, zsum, hidden_ref, eid_ref, rw_ref, isem, lsem, wsem, ssem, rsem,
):
    ep, tp = lax.axis_index("ep"), lax.axis_index("tp")
    z, x = ep // NX, ep % NX
    y, core = tp // 2, tp % 2
    other = 1 - core

    def dev(dz=0, dx=0, dy=0, c=None):
        c = core if c is None else c
        return (((z + dz) % NZ) * NX + (x + dx) % NX, ((y + dy) % NY) * 2 + c)

    inputs = [
        pltpu.make_async_copy(hidden_in, hidden_ref, isem.at[0]),
        pltpu.make_async_copy(hidden_in.at[core], hbuf.at[core, 0, 0:BLK, 0:HALF], isem.at[1]),
        pltpu.make_async_copy(gain_in, gbuf.at[tp], isem.at[2]),
        pltpu.make_async_copy(eid_in, eid_ref, isem.at[3]),
        pltpu.make_async_copy(rw_in, rw_ref, isem.at[4]),
    ]
    for cp in inputs:
        cp.start()

    barrier = pltpu.get_barrier_semaphore()
    peers = [dev(dz=o, c=c) for o in range(1, NZ) for c in range(2)] + [dev(c=other)]
    peers += [dev(dy=o, c=c) for o in range(1, NY) for c in range(2)]
    peers += [dev(dx=o) for o in range(1, NX)]
    for peer in peers:
        pl.semaphore_signal(barrier, inc=1, device_id=peer, device_id_type=MESH)

    def group(key):
        return GROUPS.index(key[0] + str(key[2]) if key[0] in RINGS + ("zs",) else key[0])

    def push(src, dst, key, to, add=0):
        i = IDS.at(*key) + add
        sem = ssem.at[group(key)]
        if key[0] == "w":
            sem = wsem.at[key[1]]
        pltpu.make_async_remote_copy(
            src_ref=src, dst_ref=dst, send_sem=sem, recv_sem=rsem.at[i], device_id=to, device_id_type=MESH
        ).start()

    def sent(ref, sem):
        pltpu.make_async_remote_copy(
            src_ref=ref, dst_ref=ref, send_sem=sem, recv_sem=rsem.at[0], device_id=dev(c=other), device_id_type=MESH
        ).wait_send()

    def arrive(dst, key, add=0):
        i = IDS.at(*key) + add
        pltpu.make_async_remote_copy(
            src_ref=dst, dst_ref=dst, send_sem=ssem.at[0], recv_sem=rsem.at[i], device_id=dev(c=other), device_id_type=MESH
        ).wait_recv()

    def lanes(first):
        return pl.ds(pl.multiple_of(first + core * 128, 128), 128)

    weights = []
    for e in range(2):
        weights.append((gate_ref.at[e], wgu.at[:, lanes(e * 256)]))
        weights.append((up_ref.at[e], wgu.at[:, lanes(512 + e * 256)]))
    weights.append((sgate_ref, wsgu.at[:, lanes(0)]))
    weights.append((sup_ref, wsgu.at[:, lanes(256)]))
    for e in range(2):
        weights.append((down_ref.at[e], wd.at[lanes(e * 256), :]))
    weights.append((sdown_ref, wsd.at[lanes(0), :]))
    local = [pltpu.make_async_copy(s, d, lsem.at[k]) for k, (s, d) in enumerate(weights)]
    def live_slots(shape, dim):
        slot = lax.broadcasted_iota(jnp.int32, shape, dim)
        seq_len = jnp.zeros(shape, jnp.int32)
        for q in range(4):
            seq_len = jnp.where(slot // 8 == q, len_ref[q], seq_len)
        return slot % 8 < seq_len

    with jax.named_scope("inputs"):
        for cp in inputs[:3]:
            cp.wait()
    for cp in local:
        cp.start()

    with jax.named_scope("barrier"):
        pl.semaphore_wait(barrier, len(peers))

    for o in (1, 7, 2, 6, 3, 5, 4):
        p = POS[(-o) % NZ]
        if o == 1:
            push(hidden_ref.at[other], hbuf.at[core, 0, 0:BLK, 0:HALF], ("zp",), dev(c=other), core)
        if p not in RELAYED:
            for c in range(2):
                push(hidden_ref.at[c], hbuf.at[core, p, 0:BLK, 0:HALF], ("z", p, 0), dev(dz=o, c=c), core)
    for k, (s, d) in enumerate(weights):
        if k < 4:
            push(s, d, ("w", k), dev(c=other))
    for o in range(NY):
        for c in range(2):
            if o > 0:
                push(gbuf.at[tp], gbuf.at[tp], ("gain",), dev(dy=o, c=c))
    push(gbuf.at[tp], gbuf.at[tp], ("gain",), dev(c=other))
    for k, (s, d) in enumerate(weights):
        if k >= 4:
            push(s, d, ("w", k), dev(c=other))

    def bslice(ref, p, h, r):
        if h == 0:
            return ref.at[h, p, 0:BLK, r * HALF : (r + 1) * HALF]
        return ref.at[h, p, r * BLK : (r + 1) * BLK, 0:HALF]

    def cslice(ref, p, h, r):
        if h == 0:
            return ref.at[h, p, r * BLK : (r + 1) * BLK, :]
        return ref.at[h, p, :, r * HALF : (r + 1) * HALF]

    def pair(view, ref, p, h):
        if view is bslice:
            return ref.at[h, p, 0 : 2 * BLK, 0:HALF] if h == 1 else ref.at[h, p, 0:BLK, 0 : 2 * HALF]
        return ref.at[h, p, 0 : 2 * BLK, :] if h == 0 else ref.at[h, p, :, 0 : 2 * HALF]

    def along(stage, h, step):
        on_y = (stage == "b") == (h == 0)
        return dev(dy=step % NY) if on_y else dev(dx=step % NX)

    def ring_first(view, stage, key, p, h, ref):
        push(view(ref, p, h, 0), view(ref, p, h, 3), (key, p, h, 3), along(stage, h, 1))
        push(view(ref, p, h, 0), view(ref, p, h, 1), (key, p, h, 1), along(stage, h, -1))
        if stage == "b" and p in DIRECT_OUT:
            push(view(ref, p, h, 0), view(ref, p, h, 2), (key, p, h, 2), along(stage, h, 2))

    def ring_forward(view, stage, key, p, h, ref):
        near, step = (3, 1) if p % 2 == 0 else (1, -1)
        arrive(view(ref, p, h, near), (key, p, h, near))
        if stage == "c" or p not in DIRECT_OUT:
            push(view(ref, p, h, near), view(ref, p, h, 2), (key, p, h, 2), along(stage, h, step))

    def ring_done(view, key, p, h, ref):
        arrive(pair(view, ref, p, h), (key, p, h, 2))

    def rslice(p, r):
        return rbuf.at[p, r * BLK : (r + 1) * BLK, :]

    def route_start():
        for cp in inputs[3:]:
            cp.wait()
        expert = lax.broadcasted_iota(jnp.int32, (128, 32), 0)
        mix = jnp.zeros((128, 32), F32)
        for k in range(8):
            mix = mix + jnp.where(eid_ref[k : k + 1, :] == expert % 64, rw_ref[k : k + 1, :], 0.0)
        mix = jnp.where(live_slots((128, 32), 1), mix, 0.0)
        high = mix.astype(BF16).astype(F32)
        terms = jnp.where(expert < 64, high, mix - high).T
        rown[...] = terms.reshape(2, BLK, 128).astype(BF16)
        rbuf[0, 0:BLK, :] = rown[core]
        for o in range(1, NZ):
            push(rown.at[core], rbuf.at[POS[-o % NZ], 0:BLK, :], ("zr", POS[-o % NZ]), dev(dz=o))

    def route_a(p):
        if p > 0:
            arrive(rslice(p, 0), ("zr", p))
        push(rslice(p, 0), rslice(p, 3), ("br", p, 3), dev(dx=1))
        push(rslice(p, 0), rslice(p, 1), ("br", p, 1), dev(dx=3))

    def route_b(p):
        near, step = (3, 1) if p % 2 == 0 else (1, 3)
        arrive(rslice(p, near), ("br", p, near))
        push(rslice(p, near), rslice(p, 2), ("br", p, 2), dev(dx=step))

    def route_c(p):
        arrive(rbuf.at[p, 0 : 2 * BLK, :], ("br", p, 2))

    def gather_a(p, h):
        if p > 0:
            arrive(hbuf.at[h, p, 0:BLK, 0:HALF], ("z", p, h))
        elif h == FIRST_HALF:
            arrive(hbuf.at[other, 0, 0:BLK, 0:HALF], ("zp",), other)
        ring_first(bslice, "b", "ab", p, h, hbuf)

    def gather_b(p, h):
        ring_forward(bslice, "b", "ab", p, h, hbuf)

    def relay(h, slots):
        for p in RELAYED:
            for r in slots:
                push(cslice(hbuf, 0, h, r), cslice(hbuf, p, h, r), ("zf", p, h), dev(dz=-SEQ[p] % NZ))

    def gather_c(p, h):
        ring_done(bslice, "ab", p, h, hbuf)
        ring_first(cslice, "c", "ac", p, h, hbuf)
        if p == 0:
            relay(h, (0,))

    def gather_d(p, h):
        ring_forward(cslice, "c", "ac", p, h, hbuf)
        if p == 0:
            relay(h, (3,))

    def gather_e(p, h):
        if p in RELAYED:
            arrive(hbuf.at[h, p], ("zf", p, h))
            return
        ring_done(cslice, "ac", p, h, hbuf)
        if p == 0:
            relay(h, (1, 2))

    def weight_ready(ks):
        for k in ks:
            local[k].wait()
            arrive(partner[k], ("w", k))

    def plan_partner():
        def lo(first):
            return pl.ds(pl.multiple_of(first + other * 128, 128), 128)

        out = []
        for e in range(2):
            out += [wgu.at[:, lo(e * 256)], wgu.at[:, lo(512 + e * 256)]]
        out += [wsgu.at[:, lo(0)], wsgu.at[:, lo(256)]]
        out += [wd.at[lo(e * 256), :] for e in range(2)]
        return out + [wsd.at[lo(0), :]]

    partner = plan_partner()

    def dot(a, b):
        return jnp.dot(a, b, preferred_element_type=F32)

    def columns(h, r):
        return pl.ds(pl.multiple_of(((y + r) % NY) * 1024 + h * HALF, HALF), HALF)

    def silu(v):
        return v / (1.0 + jnp.exp(-v))

    firsts = {letter: next(n for n in ORDER if n[0] == letter) for letter in "nmv"}

    def normalise(p):
        g = next(k for k, planes in enumerate(GROUPS_OF) if p in planes)
        offset = GROUPS_OF[g].index(p) * 64
        if firsts["n"] == f"n{p}":
            arrive(gbuf.at[0:7], ("gain",))

        def block(b, carry):
            at = pl.ds(pl.multiple_of(b * BLK, BLK), BLK)
            to = pl.ds(pl.multiple_of(offset + b * BLK, BLK), BLK)
            squares = jnp.zeros((BLK, HALF), F32)
            for h in range(2):
                for r in range(NY):
                    v = hbuf[h, p, at, r * HALF : (r + 1) * HALF].astype(F32)
                    squares = squares + v * v
            scale = lax.rsqrt(jnp.sum(squares, axis=1, keepdims=True) / 4096.0 + EPS)
            for h in range(2):
                for r in range(NY):
                    v = hbuf[h, p, at, r * HALF : (r + 1) * HALF].astype(F32)
                    gain = gbuf[((y + r) % NY) * 2 + h]
                    hn[g, to, columns(h, r)] = (v * scale * gain).astype(BF16)
            return carry

        lax.fori_loop(0, 4, block, 0)

    def hidden_units(g, e):
        if firsts["m"] == f"m{g}{e}":
            weight_ready(range(0, 4))
        route = jnp.concatenate([rbuf[p] for p in GROUPS_OF[g]], axis=0)
        pick_row = lax.broadcasted_iota(jnp.int32, (128, 256), 0) % 64
        pick = jnp.where(pick_row == ep * 2 + e, 1.0, 0.0).astype(BF16)
        share = dot(route, pick)
        gate = dot(hn[g], wgu[:, e * 256 : (e + 1) * 256])
        up = dot(hn[g], wgu[:, 512 + e * 256 : 768 + e * 256])
        inner[g, :, e * 256 : (e + 1) * 256] = (silu(gate) * up * share).astype(BF16)

    def shared_units():
        weight_ready(range(4, 6))
        g = next(k for k, planes in enumerate(GROUPS_OF) if 0 in planes)
        own = hn[g, 0:BLK, :]
        shared[...] = (silu(dot(own, wsgu[:, 0:256])) * dot(own, wsgu[:, 256:512])).astype(BF16)

    def outputs(g, h):
        if firsts["v"] == f"v{g}{h}":
            weight_ready(range(6, 9))
        for r in range(NY):
            part = dot(inner[g], wd[:, columns(h, r)])
            cols = slice(r * HALF, (r + 1) * HALF)
            for n, p in enumerate(GROUPS_OF[g]):
                pbuf[h, p, :, cols] = part[n * 64 : (n + 1) * 64].astype(BF16)
                if p == 0:
                    extra = dot(shared[...], wsd[:, columns(h, r)])
                    pbuf[h, 0, 0:BLK, cols] = (part[0:BLK] + extra).astype(BF16)
        for p in GROUPS_OF[g]:
            if p in RELAYED:
                for r in (2, 3, 1, 0):
                    push(cslice(pbuf, p, h, r), cslice(zsum, p - 1, h, r), ("zs", r, h, p), dev(dz=SEQ[p]))

    def relayed(h, r):
        for p in RELAYED:
            arrive(cslice(zsum, p - 1, h, r), ("zs", r, h, p))
        mine = cslice(pbuf, 0, h, r)
        total = mine[...].astype(F32)
        for p in RELAYED:
            total = total + cslice(zsum, p - 1, h, r)[...].astype(F32)
        mine[...] = total.astype(BF16)

    def land(stage, p, h, r):
        if stage == "b":
            return fb.at[h, p, r - 1]
        return (fc0 if h == 0 else fc1).at[p, r - 1]

    def sum_first(view, stage, key, p, h):
        near, step = (1, 1) if p % 2 == 0 else (3, -1)
        if stage == "b" and p in DIRECT_BACK:
            for r in (2, 1, 3):
                push(view(pbuf, p, h, r), land(stage, p, h, 4 - r), (key, p, h, 1), along(stage, h, r))
            return
        push(view(pbuf, p, h, 2), land(stage, p, h, 2), (key, p, h, 2), along(stage, h, step))
        push(view(pbuf, p, h, 4 - near), land(stage, p, h, near), (key, p, h, near), along(stage, h, -step))

    def sum_forward(view, stage, key, p, h):
        near, step = (1, 1) if p % 2 == 0 else (3, -1)
        if stage == "b" and p in DIRECT_BACK:
            return
        arrive(land(stage, p, h, 2), (key, p, h, 2))
        mine = view(pbuf, p, h, near)
        mine[...] = (mine[...].astype(F32) + land(stage, p, h, 2)[...].astype(F32)).astype(BF16)
        push(mine, land(stage, p, h, 4 - near), (key, p, h, 4 - near), along(stage, h, step))

    def sum_last(view, stage, key, p, h):
        whole = fb.at[h, p] if stage == "b" else (fc0 if h == 0 else fc1).at[p]
        direct = stage == "b" and p in DIRECT_BACK
        arrive(whole if direct else whole.at[0:2], (key, p, h, 1))
        mine = view(pbuf, p, h, 0)
        total = mine[...].astype(F32)
        for r in (1, 2, 3) if direct else (1, 3):
            total = total + land(stage, p, h, r)[...].astype(F32)
        mine[...] = total.astype(BF16)

    def sum_r(p, h):
        sum_first(cslice, "c", "rc", p, h)

    def sum_s(p, h):
        sum_forward(cslice, "c", "rc", p, h)

    def sum_t(p, h):
        sum_last(cslice, "c", "rc", p, h)
        sum_first(bslice, "b", "rb", p, h)

    def sum_u(p, h):
        sum_forward(bslice, "b", "rb", p, h)

    def sum_w(p, h):
        sum_last(bslice, "b", "rb", p, h)
        dz = SEQ[p]
        q = POS[(-dz) % NZ]
        if p > 0:
            push(pbuf.at[h, p, 0:BLK, 0:HALF], zb.at[q, core], ("rz",), dev(dz=dz, c=h))
        elif h == LAST_HALF:
            zb[0, core] = pbuf[core, 0, 0:BLK, 0:HALF]
            push(pbuf.at[other, 0, 0:BLK, 0:HALF], zb.at[0, core], ("rzp",), dev(c=other))

    steps = dict(y=route_start, i=route_a, j=route_b, k=route_c, a=gather_a, b=gather_b, c=gather_c, d=gather_d, e=gather_e)
    steps |= dict(n=normalise, m=hidden_units, x=shared_units, v=outputs, q=relayed, r=sum_r, s=sum_s, t=sum_t, u=sum_u, w=sum_w)
    for name in ORDER:
        with jax.named_scope(name):
            steps[name[0]](*[int(digit) for digit in name[1:]])

    with jax.named_scope("final"):
        arrive(zb.at[1 : len(PLANES)], ("rz",))
        arrive(zb.at[0, other], ("rzp",))
    live = live_slots((2 * BLK, HALF), 0)
    for c in range(2):
        total = zb[0, c].astype(F32)
        for p in PLANES[1:]:
            total = total + zb[p, c].astype(F32)
        alive = live[c * BLK : (c + 1) * BLK]
        out_ref[c] = jnp.where(alive, total, 0.0).astype(BF16)
    with jax.named_scope("drain"):
        n = len(PLANES)
        rings = {"zp": zb.at[0, 0], "rzp": zb.at[0, 0], "z": zb.at[1:n], "rz": zb.at[1:n]}
        rings |= {"zr": rbuf.at[0:7, 0:BLK, :], "br": rbuf.at[:, 0:48, :], "gain": gbuf.at[0:7]}
        for h in range(2):
            rings |= {f"ab{h}": fb.at[h, 0:n], f"rb{h}": fb.at[h, 0:n]}
            rings |= {f"ac{h}": (fc0, fc1)[h].at[0:n], f"rc{h}": (fc0, fc1)[h].at[0:n]}
            if RELAYED:
                rings[f"zs{h}"] = hbuf.at[h, 0 : len(RELAYED)]
        if RELAYED:
            rings["zf"] = hbuf.at[:, 0 : len(RELAYED)]
        for name, ref in rings.items():
            sent(ref, ssem.at[GROUPS.index(name)])
        for k, (s, _) in enumerate(weights):
            sent(s, wsem.at[k])


def body(hidden, norm_gain, expert_ids, route_weights, lengths, gate_proj, up_proj, down_proj, sgate, sup, sdown):
    vmem = pl.BlockSpec(memory_space=pltpu.VMEM)
    anywhere = pl.BlockSpec(memory_space=pltpu.HBM)
    n = IDS.count
    out = pl.pallas_call(
        kernel,
        out_shape=jax.ShapeDtypeStruct((2, BLK, HALF), BF16),
        in_specs=[anywhere] * 4 + [pl.BlockSpec(memory_space=pltpu.SMEM)] + [anywhere] * 6,
        out_specs=vmem,
        scratch_shapes=[
            pltpu.VMEM((2, NZ, 64, 2048), BF16),
            pltpu.VMEM((2, NZ, 64, 2048), BF16),
            pltpu.VMEM((NZ, 64, 128), BF16),
            pltpu.VMEM((2, BLK, 128), BF16),
            pltpu.VMEM((8, 1, HALF), F32),
            pltpu.VMEM((4, 128, 4096), BF16),
            pltpu.VMEM((4, 128, 512), BF16),
            pltpu.VMEM((BLK, 256), BF16),
            pltpu.VMEM((4096, 1024), BF16),
            pltpu.VMEM((512, 4096), BF16),
            pltpu.VMEM((4096, 512), BF16),
            pltpu.VMEM((256, 4096), BF16),
            pltpu.VMEM((NZ, 3, BLK, 2048), BF16),
            pltpu.VMEM((NZ, 3, 64, HALF), BF16),
            pltpu.VMEM((2, NZ, 3, BLK, HALF), BF16),
            pltpu.VMEM((NZ, 2, BLK, HALF), BF16),
            pltpu.VMEM((2, 2, 64, 2048), BF16),
            pltpu.VMEM((2, BLK, HALF), BF16),
            pltpu.VMEM((8, 32), jnp.int32),
            pltpu.VMEM((8, 32), F32),
            pltpu.SemaphoreType.DMA((5,)),
            pltpu.SemaphoreType.DMA((9,)),
            pltpu.SemaphoreType.DMA((9,)),
            pltpu.SemaphoreType.DMA((len(GROUPS),)),
            pltpu.SemaphoreType.DMA((n,)),
        ],
        compiler_params=pltpu.CompilerParams(
            collective_id=0, has_side_effects=True, vmem_limit_bytes=60 * 1024 * 1024
        ),
    )(
        hidden.reshape(2, BLK, HALF),
        norm_gain.reshape(1, HALF),
        expert_ids.T,
        route_weights.T,
        lengths,
        gate_proj,
        up_proj,
        down_proj,
        sgate,
        sup,
        sdown,
    )
    return out.reshape(2 * BLK, HALF)


def solution(mesh):
    placed = (
        P("ep", "tp"),
        P("tp"),
        P("ep", None),
        P("ep", None),
        P("ep"),
        P("ep", None, "tp"),
        P("ep", None, "tp"),
        P("ep", "tp", None),
        P(None, "tp"),
        P(None, "tp"),
        P("tp", None),
    )
    return jax.shard_map(body, mesh=mesh, in_specs=placed, out_specs=P("ep", "tp"), check_vma=False)
```
